32 devices in a mesh: kv: 16 (over z, y, x), tp: 2 (over core).
Axes of the slice: x: 2, y: 2, z: 4, core: 2. Of those that a mesh axis runs over, the one named last changes fastest.
Arguments:
- tokens: bfloat16 [256, 2048], P('kv', 'tp'), may hold values from -20 to 20
- norm_gain: float32 [2048], replicated, may hold values from 0.1 to 1.9
- w_query: bfloat16 [2048, 1024], P(None, 'tp'), may hold values from -0.125 to 0.125
- w_key: bfloat16 [2048, 1024], P(None, 'tp'), may hold values from -0.125 to 0.125
- w_value: bfloat16 [2048, 1024], P(None, 'tp'), may hold values from -0.125 to 0.125
- w_outgate: bfloat16 [2048, 1024], P(None, 'tp'), may hold values from -0.125 to 0.125
- w_input_gate: bfloat16 [2048, 8], replicated, may hold values from -0.125 to 0.125
- w_forget_gate: bfloat16 [2048, 8], replicated, may hold values from -0.125 to 0.125
- memory: float32 [256, 8, 128, 128], P('kv', 'tp'), may hold values from -6 to 6
- normalizer: float32 [256, 8, 128], P('kv', 'tp'), may hold values from -6 to 6
- memory_max: float32 [256, 8], P('kv', 'tp'), may hold values from -2 to 300
- w_output: bfloat16 [1024, 2048], P(None, 'tp'), may hold values from -0.1875 to 0.1875
- ffn_gain: float32 [2048], P('tp'), may hold values from 0.1 to 1.9
- w_gate: bfloat16 [2048, 5632], P('tp', 'kv'), may hold values from -0.125 to 0.125
- w_up: bfloat16 [2048, 5632], P('tp', 'kv'), may hold values from -0.125 to 0.125
- w_down: bfloat16 [5632, 2048], P('kv', 'tp'), may hold values from -0.078125 to 0.078125
Outputs:
- result: bfloat16 [256, 2048], P('kv', 'tp')
- new_memory: float32 [256, 8, 128, 128], P('kv', 'tp')
- new_normalizer: float32 [256, 8, 128], P('kv', 'tp')
- new_max: float32 [256, 8], P('kv', 'tp')
The draws below stay inside these ranges and needn't reach their ends.
All inputs are finite; a program needn't handle non-finite values.
Results may differ from the reference program's by a relative error of at most 0.013.
Values may be sent and summed in bfloat16 or wider, within the bound.
No kernel may reach another device: no remote copies, remote signals or barrier semaphores. Data moves between devices by JAX's collectives and lax.ppermute only.
A program may use at most 64 MiB of HBM per device.

```python
import jax
import jax.numpy as jnp
from jax import lax

D = 2048
HEADS = 8
HEAD_DIM = 128
INNER = 1024
FF = 5632
BATCH = 256


def draw_tokens(key, part):
    key_list = jax.random.split(jax.random.fold_in(key, 11), 3)
    col_pos = jnp.arange(D, dtype=jnp.float32) / (D - 1)
    col_jitter = jnp.exp(jax.random.uniform(key_list[2], (D,), jnp.float32, jnp.log(0.7), jnp.log(1.4)))
    base_draw = jnp.clip(jax.random.normal(key_list[0], (BATCH, D), jnp.float32), -4.0, 4.0)
    rise_curve = 0.6 * jnp.exp(col_pos * jnp.log(3.0))
    row_factor = jnp.exp(jax.random.uniform(key_list[1], (BATCH,), jnp.float32, jnp.log(0.5), jnp.log(2.0)))
    full_draw = base_draw * row_factor[:, None] * (rise_curve * col_jitter)[None, :]
    return jnp.clip(full_draw, -20.0, 20.0).astype(jnp.bfloat16)


def draw_memory_max(key, part):
    key_list = jax.random.split(jax.random.fold_in(key, 23), 1)
    base_draw = jax.random.uniform(key_list[0], (BATCH, HEADS), jnp.float32, -2.0, 2.0)
    return base_draw.astype(jnp.float32)


def shard_levels(own_key, extent, cuts, low, largest):
    loudness, own = 1.0, jax.random.fold_in(own_key, 6)
    for position, blocks in cuts:
        draws = jnp.exp(jax.random.uniform(jax.random.fold_in(own, position), (blocks,), jnp.float32, low / len(cuts), largest / len(cuts)))
        loudness = loudness * jnp.repeat(draws, extent[position] // blocks).reshape([-1 if axis == position else 1 for axis in range(len(extent))])
    return loudness


def scatter_about(rng, dims, scale, reach, pieces=(), held_as=jnp.bfloat16):
    drawn = scale * jax.random.normal(rng, dims, jnp.float32)
    if pieces:
        drawn = drawn * shard_levels(rng, dims, pieces, -0.22, 0.18)
    return jnp.clip(drawn, -reach, reach).astype(held_as)


def setup_inputs(seed: int = 0) -> dict:
    seeds = jax.random.split(jax.random.key(seed), 17)
    tokens = draw_tokens(jax.random.fold_in(seeds[16], 71), 0)
    norm_gain = jnp.clip(1.0 + 0.18 * jax.random.normal(seeds[1], (D,), jnp.float32), 0.1, 1.9)
    w_query = scatter_about(seeds[2], (D, INNER), D ** -0.5, 0.125, ((1, 2),))
    w_key = scatter_about(seeds[3], (D, INNER), D ** -0.5, 0.125, ((1, 2),))
    w_value = scatter_about(seeds[4], (D, INNER), D ** -0.5, 0.125, ((1, 2),))
    w_outgate = scatter_about(seeds[5], (D, INNER), D ** -0.5, 0.125, ((1, 2),))
    w_input_gate = scatter_about(seeds[6], (D, HEADS), D ** -0.5, 0.125)
    w_forget_gate = scatter_about(seeds[7], (D, HEADS), D ** -0.5, 0.125)
    memory = scatter_about(seeds[8], (BATCH, HEADS, HEAD_DIM, HEAD_DIM), 1.0, 6.0, ((0, 16), (1, 2)), jnp.float32)
    normalizer = scatter_about(seeds[9], (BATCH, HEADS, HEAD_DIM), 1.0, 6.0, ((0, 16), (1, 2)), jnp.float32)
    memory_max = draw_memory_max(jax.random.fold_in(seeds[16], 71), 0)
    w_output = scatter_about(seeds[11], (INNER, D), INNER ** -0.5, 0.1875, ((1, 2),))
    ffn_gain = jnp.clip(1.0 + 0.18 * jax.random.normal(seeds[12], (D,), jnp.float32), 0.1, 1.9)
    w_gate = scatter_about(seeds[13], (D, FF), D ** -0.5, 0.125, ((0, 2), (1, 16)))
    w_up = scatter_about(seeds[14], (D, FF), D ** -0.5, 0.125, ((0, 2), (1, 16)))
    w_down = scatter_about(seeds[15], (FF, D), FF ** -0.5, 0.078125, ((0, 16), (1, 2)))
    return dict(tokens=tokens, norm_gain=norm_gain, w_query=w_query, w_key=w_key, w_value=w_value, w_outgate=w_outgate, w_input_gate=w_input_gate, w_forget_gate=w_forget_gate, memory=memory, normalizer=normalizer, memory_max=memory_max, w_output=w_output, ffn_gain=ffn_gain, w_gate=w_gate, w_up=w_up, w_down=w_down)


def reference(tokens, norm_gain, w_query, w_key, w_value, w_outgate, w_input_gate, w_forget_gate, memory, normalizer, memory_max, w_output, ffn_gain, w_gate, w_up, w_down):
    tokens_f = tokens.astype(jnp.float32)
    row_scale = lax.rsqrt(lax.optimization_barrier(jnp.mean(tokens_f * tokens_f, axis=-1, keepdims=True)) + 1e-06)
    normed = (tokens_f * row_scale * norm_gain).astype(jnp.bfloat16)

    def project(weight):
        return jnp.dot(normed, weight, preferred_element_type=jnp.float32).reshape(BATCH, HEADS, HEAD_DIM)
    queries = project(w_query) * HEAD_DIM ** (-0.5)
    key_vec = project(w_key)
    values = project(w_value)
    outgate = project(w_outgate)
    igate = jnp.dot(normed, w_input_gate, preferred_element_type=jnp.float32)
    lforget = jax.nn.log_sigmoid(jnp.dot(normed, w_forget_gate, preferred_element_type=jnp.float32))
    new_max = jnp.maximum(lforget + memory_max, igate)
    keep_weight = jnp.exp(lforget + memory_max - new_max)
    admit_weight = jnp.exp(igate - new_max)
    new_memory = keep_weight[..., None, None] * memory + admit_weight[..., None, None] * (key_vec[..., :, None] * values[..., None, :])
    new_normalizer = keep_weight[..., None] * normalizer + admit_weight[..., None] * key_vec
    numerator = jnp.einsum('bhd,bhdv->bhv', queries, new_memory, precision=lax.Precision.HIGHEST)
    denominator = lax.optimization_barrier(jnp.sum(queries * new_normalizer, axis=-1))
    cell_out = numerator / jnp.maximum(jnp.abs(denominator), jnp.exp(-new_max))[..., None]
    head_mean = lax.optimization_barrier(jnp.mean(cell_out, axis=-1, keepdims=True))
    centered = cell_out - head_mean
    head_var = lax.optimization_barrier(jnp.mean(centered * centered, axis=-1, keepdims=True))
    mixed = (jax.nn.sigmoid(outgate) * centered * lax.rsqrt(head_var + 1e-05)).reshape(BATCH, INNER).astype(jnp.bfloat16)
    resid = (tokens_f + jnp.dot(mixed, w_output, preferred_element_type=jnp.float32)).astype(jnp.bfloat16)
    resid_f = resid.astype(jnp.float32)
    ffn_scale = lax.rsqrt(lax.optimization_barrier(jnp.mean(resid_f * resid_f, axis=-1, keepdims=True)) + 1e-06)
    ffn_in = (resid_f * ffn_gain).astype(jnp.bfloat16)
    gate_act = ffn_scale * jnp.dot(ffn_in, w_gate, preferred_element_type=jnp.float32)
    up_act = ffn_scale * jnp.dot(ffn_in, w_up, preferred_element_type=jnp.float32)
    hidden = (jax.nn.silu(gate_act) * up_act).astype(jnp.bfloat16)
    result = (resid_f + jnp.dot(hidden, w_down, preferred_element_type=jnp.float32)).astype(jnp.bfloat16)
    return (result, new_memory, new_normalizer, new_max)
```

```python
import jax
import jax.numpy as jnp
from jax import lax
from jax.sharding import PartitionSpec as P

BF16 = jnp.bfloat16
F32 = jnp.float32


def shifted(x, axis, size, step):
    return lax.ppermute(x, axis, [(i, (i + step) % size) for i in range(size)])


def gather_columns(x, axis, size):
    if size != 2:
        return lax.all_gather(x, axis, axis=1, tiled=True)
    other = shifted(x, axis, size, 1)
    first = lax.axis_index(axis) == 0
    return jnp.concatenate([jnp.where(first, x, other), jnp.where(first, other, x)], axis=1)


def gather_rows(x, axis, size):
    copies = jnp.broadcast_to(x[None], (size,) + x.shape)
    return lax.all_to_all(copies, axis, 0, 0).reshape(size * x.shape[0], x.shape[1])


def make(kv, tp):
    def per_device(
        tokens,
        norm_gain,
        w_query,
        w_key,
        w_value,
        w_outgate,
        w_input_gate,
        w_forget_gate,
        memory,
        normalizer,
        memory_max,
        w_output,
        ffn_gain,
        w_gate,
        w_up,
        w_down,
    ):
        rows, own_channels = tokens.shape
        heads, head_dim = memory.shape[1], memory.shape[2]
        channels = own_channels * tp
        hidden_units = w_gate.shape[1]

        full_rows = gather_columns(tokens, "tp", tp).astype(F32)
        row_scale = lax.rsqrt(jnp.mean(full_rows * full_rows, axis=-1, keepdims=True) + 1e-06)
        normed = (full_rows * row_scale * norm_gain).astype(BF16)

        def project(weight):
            return jnp.dot(normed, weight, preferred_element_type=F32)

        def by_head(x):
            return x.reshape(rows, heads, head_dim)

        queries = by_head(project(w_query)) * head_dim ** (-0.5)
        key_vec = by_head(project(w_key))
        values = by_head(project(w_value))
        outgate = by_head(project(w_outgate))
        first_head = lax.axis_index("tp") * heads
        igate = lax.dynamic_slice_in_dim(project(w_input_gate), first_head, heads, 1)
        forget_pre = lax.dynamic_slice_in_dim(project(w_forget_gate), first_head, heads, 1)
        lforget = jax.nn.log_sigmoid(forget_pre)
        new_max = jnp.maximum(lforget + memory_max, igate)
        keep = jnp.exp(lforget + memory_max - new_max)
        admit = jnp.exp(igate - new_max)
        new_normalizer = keep[..., None] * normalizer + admit[..., None] * key_vec
        old_part = jnp.einsum("bhd,bhdv->bhv", queries, memory, precision=lax.Precision.HIGHEST)
        query_key = jnp.sum(queries * key_vec, axis=-1)
        numerator = keep[..., None] * old_part + (admit * query_key)[..., None] * values
        denominator = jnp.sum(queries * new_normalizer, axis=-1)
        cell_out = numerator / jnp.maximum(jnp.abs(denominator), jnp.exp(-new_max))[..., None]
        head_mean = jnp.mean(cell_out, axis=-1, keepdims=True)
        centered = cell_out - head_mean
        head_var = jnp.mean(centered * centered, axis=-1, keepdims=True)
        mixed = jax.nn.sigmoid(outgate) * centered * lax.rsqrt(head_var + 1e-05)
        mixed = mixed.reshape(rows, heads * head_dim).astype(BF16)

        branch_out = jnp.dot(gather_columns(mixed, "tp", tp), w_output, preferred_element_type=F32)
        resid = (tokens.astype(F32) + branch_out).astype(BF16)
        every_row = gather_rows(resid, "kv", kv)
        new_memory = keep[..., None, None] * memory + admit[..., None, None] * (
            key_vec[..., :, None] * values[..., None, :]
        )

        every_f = every_row.astype(F32)
        squares = jnp.sum(every_f * every_f, axis=-1, keepdims=True)
        squares_hi = squares.astype(BF16)
        squares_lo = (squares - squares_hi.astype(F32)).astype(BF16)
        ffn_in = (every_f * ffn_gain).astype(BF16)
        gate_part = jnp.dot(ffn_in, w_gate, preferred_element_type=F32)
        up_part = jnp.dot(ffn_in, w_up, preferred_element_type=F32)
        packed = jnp.concatenate([gate_part.astype(BF16), up_part.astype(BF16), squares_hi, squares_lo], axis=1)
        for step in range(1, tp):
            other = shifted(packed, "tp", tp, step).astype(F32)
            gate_part = gate_part + other[:, :hidden_units]
            up_part = up_part + other[:, hidden_units : 2 * hidden_units]
            squares = squares + jnp.sum(other[:, 2 * hidden_units :], axis=1, keepdims=True)
        ffn_scale = lax.rsqrt(squares / channels + 1e-06)
        hidden = (jax.nn.silu(ffn_scale * gate_part) * (ffn_scale * up_part)).astype(BF16)
        down_part = jnp.dot(hidden, w_down, preferred_element_type=F32).astype(BF16)
        pieces = lax.all_to_all(down_part.reshape(kv, rows, own_channels), "kv", 0, 0)
        down_out = jnp.sum(pieces.astype(F32), axis=0)
        result = (resid.astype(F32) + down_out).astype(BF16)
        return (result, new_memory, new_normalizer, new_max)

    return per_device


def solution(mesh):
    placed = (
        P("kv", "tp"),
        P(),
        P(None, "tp"),
        P(None, "tp"),
        P(None, "tp"),
        P(None, "tp"),
        P(),
        P(),
        P("kv", "tp", None, None),
        P("kv", "tp", None),
        P("kv", "tp"),
        P(None, "tp"),
        P("tp"),
        P("tp", "kv"),
        P("tp", "kv"),
        P("kv", "tp"),
    )
    return jax.shard_map(
        make(mesh.shape["kv"], mesh.shape["tp"]),
        mesh=mesh,
        in_specs=placed,
        out_specs=(P("kv", "tp"), P("kv", "tp", None, None), P("kv", "tp", None), P("kv", "tp")),
        check_vma=False,
    )
```

```python
import functools

import jax
import jax.numpy as jnp
from jax import lax
from jax.experimental import pallas as pl
from jax.experimental.pallas import tpu as pltpu
from jax.sharding import PartitionSpec as P

BF16 = jnp.bfloat16
F32 = jnp.float32
LANES = 128
W_PARTS = 4
IN_FLIGHT = 9
CELL_VMEM = 24 * 2**20
HBM = pl.BlockSpec(memory_space=pltpu.HBM)
VMEM = pl.BlockSpec(memory_space=pltpu.VMEM)
NT = (((1,), (1,)), ((), ()))


def shifted(x, axis, size, step):
    return lax.ppermute(x, axis, [(i, (i + step) % size) for i in range(size)])


def column_pieces(x, axis, size):
    if size != 2:
        return [lax.all_gather(x, axis, axis=1, tiled=True)]
    return [x, shifted(x, axis, size, 1)]


def in_hbm(x):
    return pltpu.with_memory_space_constraint(x, pltpu.HBM)


def piece_starts(refs, axis):
    if len(refs) == 1:
        return [0]
    me, width = lax.axis_index(axis), refs[0].shape[1]
    return [pl.multiple_of(me * width, LANES), pl.multiple_of((1 - me) * width, LANES)]


def load_kernel(count, *refs):
    sources, targets, sem = refs[:count], refs[count : 2 * count], refs[-1]
    copies = [pltpu.make_async_copy(a, b, sem.at[i]) for i, (a, b) in enumerate(zip(sources, targets))]
    for copy in copies:
        copy.start()
    for copy in copies:
        copy.wait()


def load(arrays):
    return pl.pallas_call(
        functools.partial(load_kernel, len(arrays)),
        name="load",
        out_shape=[pltpu.VMEM(x.shape, x.dtype) for x in arrays],
        in_specs=[HBM] * len(arrays),
        out_specs=[VMEM] * len(arrays),
        scratch_shapes=[pltpu.SemaphoreType.DMA((len(arrays),))],
        compiler_params=pltpu.CompilerParams(vmem_limit_bytes=4 * 2**20),
        cost_estimate=pl.CostEstimate(flops=2**28, bytes_accessed=2**18, transcendentals=0),
    )(*map(in_hbm, arrays))


def cell_kernel(pieces, *refs):
    partner_refs, refs = refs[: pieces - 1], refs[pieces - 1 :]
    (own, gain, wi, wf, normalizer, old_max_t, wq, wk, wv, wo, memory, *refs) = refs
    (mixed, new_normalizer, new_max_t, keep_out, admit_out, key_out, value_out, *refs) = refs
    (full, w_buf, m_buf, old_part, w_sem, m_sem) = refs
    rows, heads, dim = normalizer.shape
    blocks = m_buf.shape[0]
    block_rows = rows // blocks
    depth = w_buf.shape[1] // W_PARTS

    w_copies = [
        [
            pltpu.make_async_copy(
                w.at[pl.ds(p * depth, depth)], w_buf.at[i, pl.ds(p * depth, depth)], w_sem.at[i, p]
            )
            for p in range(W_PARTS)
        ]
        for i, w in enumerate([wq, wk, wv, wo])
    ]
    m_copies = [
        pltpu.make_async_copy(memory.at[pl.ds(i * block_rows, block_rows)], m_buf.at[i], m_sem.at[i])
        for i in range(blocks)
    ]
    stream = w_copies[0] + m_copies + w_copies[1] + w_copies[2] + w_copies[3]
    for copy in stream[:IN_FLIGHT]:
        copy.start()
    waiting = list(stream)
    later = list(stream[IN_FLIGHT:])

    def arrive():
        waiting.pop(0).wait()
        if later:
            later.pop(0).start()

    token_refs = [own, *partner_refs]
    for ref, start in zip(token_refs, piece_starts(token_refs, "tp")):
        full[:, pl.ds(start, ref.shape[1])] = ref[...].astype(F32)
    x = full[...]
    scale = lax.rsqrt(jnp.mean(x * x, axis=1, keepdims=True) + 1e-06)
    normed = (x * scale * gain[...]).astype(BF16)

    def nt(a, b):
        return lax.dot_general(a, b, NT, preferred_element_type=F32)

    all_heads = wi.shape[0]
    me = lax.axis_index("tp")

    def own_heads(x):
        out = x[:heads]
        for i in range(1, all_heads // heads):
            out = jnp.where(me == i, x[i * heads : (i + 1) * heads], out)
        return out

    igate = own_heads(nt(wi[...], normed))
    lforget = jax.nn.log_sigmoid(own_heads(nt(wf[...], normed)))
    old_max = old_max_t[...]
    max_t = jnp.maximum(lforget + old_max, igate)
    new_max_t[...] = max_t
    keep = jnp.exp(lforget + old_max - max_t).T
    admit = jnp.exp(igate - max_t).T
    floor = jnp.exp(-max_t).T
    keep_out[...] = keep
    admit_out[...] = admit

    def project(i):
        total = None
        for p in range(W_PARTS):
            arrive()
            part = jnp.dot(
                normed[:, p * depth : (p + 1) * depth],
                w_buf[i, p * depth : (p + 1) * depth, :],
                preferred_element_type=F32,
            )
            total = part if total is None else total + part
        return total

    def head(x, h):
        return x[:, h * dim : (h + 1) * dim]

    queries = project(0) * dim ** (-0.5)
    columns = [head(queries, h).T for h in range(heads)]
    for block in range(blocks):
        arrive()
        for r in range(block_rows):
            b = block * block_rows + r
            for h in range(heads):
                part = jnp.sum(m_buf[block, r, h] * columns[h][:, b : b + 1], axis=0, keepdims=True)
                old_part[h, b : b + 1, :] = part

    keys = project(1)
    key_out[...] = keys
    scales = []
    for h in range(heads):
        q, k = head(queries, h), head(keys, h)
        kw, aw = keep[:, h : h + 1], admit[:, h : h + 1]
        norm = kw * normalizer[:, h, :] + aw * k
        new_normalizer[:, h, :] = norm
        query_key = jnp.sum(q * k, axis=1, keepdims=True)
        denominator = jnp.sum(q * norm, axis=1, keepdims=True)
        scales.append((aw * query_key, jnp.maximum(jnp.abs(denominator), floor[:, h : h + 1])))
    values = project(2)
    value_out[...] = values
    normalised = []
    for h in range(heads):
        weight, divisor = scales[h]
        numerator = keep[:, h : h + 1] * old_part[h] + weight * head(values, h)
        cell_out = numerator / divisor
        centered = cell_out - jnp.mean(cell_out, axis=1, keepdims=True)
        variance = jnp.mean(centered * centered, axis=1, keepdims=True)
        normalised.append(centered * lax.rsqrt(variance + 1e-05))
    outgate = jax.nn.sigmoid(project(3))
    for h in range(heads):
        mixed[:, h * dim : (h + 1) * dim] = (head(outgate, h) * normalised[h]).astype(BF16)


def run_cell(token_pieces, gain, wi, wf, normalizer, old_max, weights, memory):
    rows, heads, dim = normalizer.shape
    depth, inner = weights[0].shape
    blocks = 8 if rows % 8 == 0 else 1
    own, *partners = token_pieces
    flops = 2 * rows * depth * inner * 4
    return pl.pallas_call(
        functools.partial(cell_kernel, len(token_pieces)),
        name="cell",
        out_shape=[
            pltpu.VMEM((rows, inner), BF16),
            jax.ShapeDtypeStruct((rows, heads, dim), F32),
            jax.ShapeDtypeStruct((heads, rows), F32),
            pltpu.VMEM((rows, heads), F32),
            pltpu.VMEM((rows, heads), F32),
            pltpu.VMEM((rows, inner), F32),
            pltpu.VMEM((rows, inner), F32),
        ],
        in_specs=[VMEM] * (len(partners) + 6) + [HBM] * 5,
        out_specs=[VMEM] * 7,
        scratch_shapes=[
            pltpu.VMEM((rows, depth), F32),
            pltpu.VMEM((4, depth, inner), BF16),
            pltpu.VMEM((blocks, rows // blocks, heads, dim, dim), F32),
            pltpu.VMEM((heads, rows, dim), F32),
            pltpu.SemaphoreType.DMA((4, W_PARTS)),
            pltpu.SemaphoreType.DMA((blocks,)),
        ],
        compiler_params=pltpu.CompilerParams(vmem_limit_bytes=CELL_VMEM),
        cost_estimate=pl.CostEstimate(flops=flops * 64, bytes_accessed=13 * 2**20, transcendentals=0),
    )(*partners, *load([own, gain, wi, wf, normalizer, old_max.T]), *map(in_hbm, [*weights, memory]))


def out_kernel(pieces, *refs):
    mixed_refs, (tokens, w_output, resid, copies) = refs[:pieces], refs[pieces:]
    total = tokens[...].astype(F32)
    for ref, start in zip(mixed_refs, piece_starts(mixed_refs, "tp")):
        weight = w_output[pl.ds(start, ref.shape[1]), :]
        total = total + jnp.dot(ref[...], weight, preferred_element_type=F32)
    out = total.astype(BF16)
    resid[...] = out
    for i in range(copies.shape[0]):
        copies[i] = out


def run_out(mixed_pieces, tokens, w_output, kv):
    rows, width = tokens.shape
    return pl.pallas_call(
        functools.partial(out_kernel, len(mixed_pieces)),
        name="out_projection",
        out_shape=[jax.ShapeDtypeStruct((rows, width), BF16), jax.ShapeDtypeStruct((kv, rows, width), BF16)],
        in_specs=[VMEM] * (len(mixed_pieces) + 2),
        out_specs=[VMEM, VMEM],
        compiler_params=pltpu.CompilerParams(vmem_limit_bytes=24 * 2**20),
        cost_estimate=pl.CostEstimate(
            flops=2 * rows * w_output.size, bytes_accessed=2 * w_output.size, transcendentals=0
        ),
    )(*mixed_pieces, tokens, w_output)


def up_kernel(rows_ref, gain, w_gate, w_up, own, sent):
    hidden = w_gate.shape[0]
    half = own.shape[1] // 2
    x = rows_ref[...].astype(F32)
    squares = jnp.sum(x * x, axis=1, keepdims=True)
    ffn_in = (x * gain[...]).astype(BF16)
    own[...] = jnp.zeros_like(own)
    for weight, first in [(w_gate, 0), (w_up, half)]:
        own[:, first : first + hidden] = lax.dot_general(ffn_in, weight[...], NT, preferred_element_type=F32)
    lane = lax.broadcasted_iota(jnp.int32, (x.shape[0], LANES), 1)
    high = squares.astype(BF16).astype(F32)
    first = hidden // LANES * LANES
    tile = own[:, first : first + LANES]
    spot = hidden - first
    own[:, first : first + LANES] = jnp.where(lane == spot, squares, tile)
    sent[...] = own[...].astype(BF16)
    tile = jnp.where(lane == spot, high, jnp.where(lane == spot + 1, squares - high, tile))
    sent[:, first : first + LANES] = tile.astype(BF16)


def run_up(every_row, gain, w_gate, w_up):
    rows, depth = every_row.shape
    hidden = w_gate.shape[1]
    half = (hidden + 2 + LANES - 1) // LANES * LANES
    return pl.pallas_call(
        up_kernel,
        name="gate_up",
        out_shape=[jax.ShapeDtypeStruct((rows, 2 * half), F32), jax.ShapeDtypeStruct((rows, 2 * half), BF16)],
        in_specs=[VMEM] * 4,
        out_specs=[VMEM, VMEM],
        compiler_params=pltpu.CompilerParams(vmem_limit_bytes=24 * 2**20),
        cost_estimate=pl.CostEstimate(flops=4 * rows * depth * hidden, bytes_accessed=4 * 2**20, transcendentals=0),
    )(every_row, gain, w_gate.T, w_up.T)


def down_kernel(others, channels, own, *refs):
    other_refs, (w_down, out) = refs[:others], refs[others:]
    hidden = w_down.shape[0]
    half = own.shape[1] // 2
    gate, up = own[:, :half], own[:, half:]
    squares = gate[:, hidden : hidden + 1]
    for ref in other_refs:
        theirs = ref[...].astype(F32)
        gate, up = gate + theirs[:, :half], up + theirs[:, half:]
        squares = squares + theirs[:, hidden : hidden + 1] + theirs[:, hidden + 1 : hidden + 2]
    scale = lax.rsqrt(squares / channels + 1e-06)
    gate = scale * gate[:, :hidden]
    act = (gate * jax.nn.sigmoid(gate) * (scale * up[:, :hidden])).astype(BF16)
    out[...] = jnp.dot(act, w_down[...], preferred_element_type=F32).astype(BF16)


def run_down(own, others, w_down, channels):
    rows = own.shape[0]
    hidden, width = w_down.shape
    return pl.pallas_call(
        functools.partial(down_kernel, len(others), channels),
        name="down",
        out_shape=jax.ShapeDtypeStruct((rows, width), BF16),
        in_specs=[VMEM] * (2 + len(others)),
        out_specs=VMEM,
        compiler_params=pltpu.CompilerParams(vmem_limit_bytes=24 * 2**20),
        cost_estimate=pl.CostEstimate(flops=2 * rows * width * hidden, bytes_accessed=2 * 2**20, transcendentals=0),
    )(own, *others, w_down)


def make(kv, tp):
    def per_device(
        tokens,
        norm_gain,
        w_query,
        w_key,
        w_value,
        w_outgate,
        w_input_gate,
        w_forget_gate,
        memory,
        normalizer,
        memory_max,
        w_output,
        ffn_gain,
        w_gate,
        w_up,
        w_down,
    ):
        rows, own_channels = tokens.shape
        heads, head_dim = memory.shape[1], memory.shape[2]
        pieces = column_pieces(tokens, "tp", tp)
        mixed, new_normalizer, new_max_t, keep, admit, keys, values = run_cell(
            pieces,
            norm_gain[None],
            w_input_gate.T,
            w_forget_gate.T,
            normalizer,
            memory_max,
            [w_query, w_key, w_value, w_outgate],
            memory,
        )
        pieces = column_pieces(mixed, "tp", tp)
        resid, copies = run_out(pieces, tokens, w_output, kv)
        every_row = lax.all_to_all(copies, "kv", 0, 0).reshape(kv * rows, own_channels)
        by_head = (rows, heads, head_dim)
        keys, values = keys.reshape(by_head), values.reshape(by_head)
        new_memory = keep[..., None, None] * memory + admit[..., None, None] * (
            keys[..., :, None] * values[..., None, :]
        )

        own, sent = run_up(every_row, ffn_gain[None], w_gate, w_up)
        others = [shifted(sent, "tp", tp, step) for step in range(1, tp)]
        down_part = run_down(own, others, w_down, own_channels * tp)
        pieces = lax.all_to_all(down_part.reshape(kv, rows, own_channels), "kv", 0, 0)
        down_out = jnp.sum(pieces.astype(F32), axis=0)
        result = (resid.astype(F32) + down_out).astype(BF16)
        return (result, new_memory, new_normalizer, new_max_t.T)

    return per_device


def solution(mesh):
    placed = (
        P("kv", "tp"),
        P(),
        P(None, "tp"),
        P(None, "tp"),
        P(None, "tp"),
        P(None, "tp"),
        P(),
        P(),
        P("kv", "tp", None, None),
        P("kv", "tp", None),
        P("kv", "tp"),
        P(None, "tp"),
        P("tp"),
        P("tp", "kv"),
        P("tp", "kv"),
        P("kv", "tp"),
    )
    return jax.shard_map(
        make(mesh.shape["kv"], mesh.shape["tp"]),
        mesh=mesh,
        in_specs=placed,
        out_specs=(P("kv", "tp"), P("kv", "tp", None, None), P("kv", "tp", None), P("kv", "tp")),
        check_vma=False,
    )
```

```python
import functools

import jax
import jax.numpy as jnp
from jax import lax
from jax.experimental import pallas as pl
from jax.experimental.pallas import tpu as pltpu
from jax.sharding import PartitionSpec as P

BF16 = jnp.bfloat16
F32 = jnp.float32
LANES = 128
COVER = 2**36
HBM = pl.BlockSpec(memory_space=pltpu.HBM)
VMEM = pl.BlockSpec(memory_space=pltpu.VMEM)
NT = (((1,), (1,)), ((), ()))


def shifted(x, axis, size, step):
    return lax.ppermute(x, axis, [(i, (i + step) % size) for i in range(size)])


def column_pieces(x, axis, size):
    if size != 2:
        return [lax.all_gather(x, axis, axis=1, tiled=True)]
    return [x, shifted(x, axis, size, 1)]


def in_vmem(x):
    return pltpu.with_memory_space_constraint(x, pltpu.VMEM)


def in_hbm(x):
    return pltpu.with_memory_space_constraint(x, pltpu.HBM)


def piece_starts(refs, axis):
    if len(refs) == 1:
        return [0]
    me, width = lax.axis_index(axis), refs[0].shape[1]
    return [pl.multiple_of(me * width, LANES), pl.multiple_of((1 - me) * width, LANES)]


def load_kernel(count, *refs):
    sources, targets, sem = refs[:count], refs[count : 2 * count], refs[-1]
    copies = [pltpu.make_async_copy(a, b, sem.at[i]) for i, (a, b) in enumerate(zip(sources, targets))]
    for copy in copies:
        copy.start()
    for copy in copies:
        copy.wait()


def load(arrays):
    return pl.pallas_call(
        functools.partial(load_kernel, len(arrays)),
        name="load",
        out_shape=[pltpu.VMEM(x.shape, x.dtype) for x in arrays],
        in_specs=[HBM] * len(arrays),
        out_specs=[VMEM] * len(arrays),
        scratch_shapes=[pltpu.SemaphoreType.DMA((len(arrays),))],
        compiler_params=pltpu.CompilerParams(vmem_limit_bytes=4 * 2**20),
        cost_estimate=pl.CostEstimate(flops=COVER, bytes_accessed=2**18, transcendentals=0),
    )(*map(in_hbm, arrays))


def read_kernel(pieces, *refs):
    token_refs, refs = refs[:pieces], refs[pieces:]
    (gain, wi, wf, old_max_t, wq, memory, *refs) = refs
    (normed_out, query_out, old_part, keep_out, admit_out, floor_out, new_max_t, full) = refs
    rows, heads, dim = memory.shape[:3]

    for ref, start in zip(token_refs, piece_starts(token_refs, "tp")):
        full[:, pl.ds(start, ref.shape[1])] = ref[...].astype(F32)
    x = full[...]
    scale = lax.rsqrt(jnp.mean(x * x, axis=1, keepdims=True) + 1e-06)
    normed = (x * scale * gain[...]).astype(BF16)
    normed_out[...] = normed

    def nt(a, b):
        return lax.dot_general(a, b, NT, preferred_element_type=F32)

    all_heads = wi.shape[0]
    me = lax.axis_index("tp")

    def own_heads(x):
        out = x[:heads]
        for i in range(1, all_heads // heads):
            out = jnp.where(me == i, x[i * heads : (i + 1) * heads], out)
        return out

    queries = jnp.dot(normed, wq[...], preferred_element_type=F32) * dim ** (-0.5)
    query_out[...] = queries
    igate = own_heads(nt(wi[...], normed))
    lforget = jax.nn.log_sigmoid(own_heads(nt(wf[...], normed)))
    old_max = old_max_t[...]
    max_t = jnp.maximum(lforget + old_max, igate)
    new_max_t[...] = max_t
    keep_out[...] = jnp.exp(lforget + old_max - max_t).T
    admit_out[...] = jnp.exp(igate - max_t).T
    floor_out[...] = jnp.exp(-max_t).T

    columns = [queries[:, h * dim : (h + 1) * dim].T for h in range(heads)]
    for b in range(rows):
        for h in range(heads):
            part = jnp.sum(memory[b, h] * columns[h][:, b : b + 1], axis=0, keepdims=True)
            old_part[h, b : b + 1, :] = part


def run_read(token_pieces, gain, wi, wf, old_max_t, wq, memory):
    rows, heads, dim = memory.shape[:3]
    depth, inner = wq.shape
    flops = 2 * rows * depth * inner
    return pl.pallas_call(
        functools.partial(read_kernel, len(token_pieces)),
        name="read",
        out_shape=[
            pltpu.VMEM((rows, depth), BF16),
            pltpu.VMEM((rows, inner), F32),
            pltpu.VMEM((heads, rows, dim), F32),
            pltpu.VMEM((rows, heads), F32),
            pltpu.VMEM((rows, heads), F32),
            pltpu.VMEM((rows, heads), F32),
            jax.ShapeDtypeStruct((heads, rows), F32),
        ],
        in_specs=[VMEM] * (len(token_pieces) + 6),
        out_specs=[VMEM] * 7,
        scratch_shapes=[pltpu.VMEM((rows, depth), F32)],
        compiler_params=pltpu.CompilerParams(vmem_limit_bytes=16 * 2**20),
        cost_estimate=pl.CostEstimate(flops=flops * 32, bytes_accessed=6 * 2**20, transcendentals=0),
    )(*token_pieces, gain, wi, wf, old_max_t, *map(in_vmem, [wq, memory]))


def mix_kernel(*refs):
    (normed, query, old_part, keep, admit, floor, normalizer, wk, wv, wo, *refs) = refs
    (mixed, new_normalizer, key_out, value_out) = refs
    rows, heads, dim = normalizer.shape

    def head(x, h):
        return x[:, h * dim : (h + 1) * dim]

    x = normed[...]
    keys = jnp.dot(x, wk[...], preferred_element_type=F32)
    values = jnp.dot(x, wv[...], preferred_element_type=F32)
    outgate = jax.nn.sigmoid(jnp.dot(x, wo[...], preferred_element_type=F32))
    key_out[...] = keys
    value_out[...] = values
    for h in range(heads):
        q, k, v = head(query[...], h), head(keys, h), head(values, h)
        kw, aw = keep[:, h : h + 1], admit[:, h : h + 1]
        norm = kw * normalizer[:, h, :] + aw * k
        new_normalizer[:, h, :] = norm
        query_key = jnp.sum(q * k, axis=1, keepdims=True)
        denominator = jnp.sum(q * norm, axis=1, keepdims=True)
        numerator = kw * old_part[h] + (aw * query_key) * v
        cell_out = numerator / jnp.maximum(jnp.abs(denominator), floor[:, h : h + 1])
        centered = cell_out - jnp.mean(cell_out, axis=1, keepdims=True)
        variance = jnp.mean(centered * centered, axis=1, keepdims=True)
        gated = head(outgate, h) * centered * lax.rsqrt(variance + 1e-05)
        mixed[:, h * dim : (h + 1) * dim] = gated.astype(BF16)


def run_mix(normed, query, old_part, keep, admit, floor, normalizer, weights):
    rows, heads, dim = normalizer.shape
    depth, inner = weights[0].shape
    flops = 2 * rows * depth * inner * len(weights)
    return pl.pallas_call(
        mix_kernel,
        name="mix",
        out_shape=[
            pltpu.VMEM((rows, inner), BF16),
            jax.ShapeDtypeStruct((rows, heads, dim), F32),
            pltpu.VMEM((rows, inner), F32),
            pltpu.VMEM((rows, inner), F32),
        ],
        in_specs=[VMEM] * 10,
        out_specs=[VMEM] * 4,
        compiler_params=pltpu.CompilerParams(vmem_limit_bytes=16 * 2**20),
        cost_estimate=pl.CostEstimate(flops=flops * 32, bytes_accessed=6 * 2**20, transcendentals=0),
    )(normed, query, old_part, keep, admit, floor, normalizer, *map(in_vmem, weights))


def out_kernel(pieces, *refs):
    mixed_refs, (tokens, w_output, resid, copies) = refs[:pieces], refs[pieces:]
    total = tokens[...].astype(F32)
    for ref, start in zip(mixed_refs, piece_starts(mixed_refs, "tp")):
        weight = w_output[pl.ds(start, ref.shape[1]), :]
        total = total + jnp.dot(ref[...], weight, preferred_element_type=F32)
    out = total.astype(BF16)
    resid[...] = out
    for i in range(copies.shape[0]):
        copies[i] = out


def run_out(mixed_pieces, tokens, w_output, kv):
    rows, width = tokens.shape
    return pl.pallas_call(
        functools.partial(out_kernel, len(mixed_pieces)),
        name="out_projection",
        out_shape=[jax.ShapeDtypeStruct((rows, width), BF16), jax.ShapeDtypeStruct((kv, rows, width), BF16)],
        in_specs=[VMEM] * (len(mixed_pieces) + 2),
        out_specs=[VMEM, VMEM],
        compiler_params=pltpu.CompilerParams(vmem_limit_bytes=24 * 2**20),
        cost_estimate=pl.CostEstimate(
            flops=2 * rows * w_output.size, bytes_accessed=2 * w_output.size, transcendentals=0
        ),
    )(*mixed_pieces, tokens, w_output)


def up_kernel(rows_ref, gain, w_gate, w_up, own, sent):
    hidden = w_gate.shape[0]
    half = own.shape[1] // 2
    x = rows_ref[...].astype(F32)
    squares = jnp.sum(x * x, axis=1, keepdims=True)
    ffn_in = (x * gain[...]).astype(BF16)
    own[...] = jnp.zeros_like(own)
    for weight, first in [(w_gate, 0), (w_up, half)]:
        own[:, first : first + hidden] = lax.dot_general(ffn_in, weight[...], NT, preferred_element_type=F32)
    lane = lax.broadcasted_iota(jnp.int32, (x.shape[0], LANES), 1)
    high = squares.astype(BF16).astype(F32)
    first = hidden // LANES * LANES
    tile = own[:, first : first + LANES]
    spot = hidden - first
    own[:, first : first + LANES] = jnp.where(lane == spot, squares, tile)
    sent[...] = own[...].astype(BF16)
    tile = jnp.where(lane == spot, high, jnp.where(lane == spot + 1, squares - high, tile))
    sent[:, first : first + LANES] = tile.astype(BF16)


def run_up(every_row, gain, w_gate, w_up):
    rows, depth = every_row.shape
    hidden = w_gate.shape[1]
    half = (hidden + 2 + LANES - 1) // LANES * LANES
    return pl.pallas_call(
        up_kernel,
        name="gate_up",
        out_shape=[jax.ShapeDtypeStruct((rows, 2 * half), F32), jax.ShapeDtypeStruct((rows, 2 * half), BF16)],
        in_specs=[VMEM] * 4,
        out_specs=[VMEM, VMEM],
        compiler_params=pltpu.CompilerParams(vmem_limit_bytes=24 * 2**20),
        cost_estimate=pl.CostEstimate(flops=4 * rows * depth * hidden, bytes_accessed=4 * 2**20, transcendentals=0),
    )(every_row, gain, w_gate.T, w_up.T)


def down_kernel(others, channels, own, *refs):
    other_refs, (w_down, out) = refs[:others], refs[others:]
    hidden = w_down.shape[0]
    half = own.shape[1] // 2
    gate, up = own[:, :half], own[:, half:]
    squares = gate[:, hidden : hidden + 1]
    for ref in other_refs:
        theirs = ref[...].astype(F32)
        gate, up = gate + theirs[:, :half], up + theirs[:, half:]
        squares = squares + theirs[:, hidden : hidden + 1] + theirs[:, hidden + 1 : hidden + 2]
    scale = lax.rsqrt(squares / channels + 1e-06)
    gate = scale * gate[:, :hidden]
    act = (gate * jax.nn.sigmoid(gate) * (scale * up[:, :hidden])).astype(BF16)
    out[...] = jnp.dot(act, w_down[...], preferred_element_type=F32).astype(BF16)


def run_down(own, others, w_down, channels):
    rows = own.shape[0]
    hidden, width = w_down.shape
    return pl.pallas_call(
        functools.partial(down_kernel, len(others), channels),
        name="down",
        out_shape=jax.ShapeDtypeStruct((rows, width), BF16),
        in_specs=[VMEM] * (2 + len(others)),
        out_specs=VMEM,
        compiler_params=pltpu.CompilerParams(vmem_limit_bytes=24 * 2**20),
        cost_estimate=pl.CostEstimate(flops=2 * rows * width * hidden, bytes_accessed=2 * 2**20, transcendentals=0),
    )(own, *others, w_down)


def make(kv, tp):
    def per_device(
        tokens,
        norm_gain,
        w_query,
        w_key,
        w_value,
        w_outgate,
        w_input_gate,
        w_forget_gate,
        memory,
        normalizer,
        memory_max,
        w_output,
        ffn_gain,
        w_gate,
        w_up,
        w_down,
    ):
        rows, own_channels = tokens.shape
        heads, head_dim = memory.shape[1], memory.shape[2]
        own, gain, wi, wf, old_normalizer, old_max_t = load(
            [tokens, norm_gain[None], w_input_gate.T, w_forget_gate.T, normalizer, memory_max.T]
        )
        pieces = column_pieces(own, "tp", tp)
        normed, query, old_part, keep, admit, floor, new_max_t = run_read(
            pieces, gain, wi, wf, old_max_t, w_query, memory
        )
        mixed, new_normalizer, keys, values = run_mix(
            normed, query, old_part, keep, admit, floor, old_normalizer, [w_key, w_value, w_outgate]
        )
        pieces = column_pieces(mixed, "tp", tp)
        resid, copies = run_out(pieces, tokens, w_output, kv)
        every_row = lax.all_to_all(copies, "kv", 0, 0).reshape(kv * rows, own_channels)
        by_head = (rows, heads, head_dim)
        keys, values = keys.reshape(by_head), values.reshape(by_head)
        new_memory = keep[..., None, None] * memory + admit[..., None, None] * (
            keys[..., :, None] * values[..., None, :]
        )

        own, sent = run_up(every_row, ffn_gain[None], w_gate, w_up)
        others = [shifted(sent, "tp", tp, step) for step in range(1, tp)]
        down_part = run_down(own, others, w_down, own_channels * tp)
        pieces = lax.all_to_all(down_part.reshape(kv, rows, own_channels), "kv", 0, 0)
        down_out = jnp.sum(pieces.astype(F32), axis=0)
        result = (resid.astype(F32) + down_out).astype(BF16)
        return (result, new_memory, new_normalizer, new_max_t.T)

    return per_device


def solution(mesh):
    placed = (
        P("kv", "tp"),
        P(),
        P(None, "tp"),
        P(None, "tp"),
        P(None, "tp"),
        P(None, "tp"),
        P(),
        P(),
        P("kv", "tp", None, None),
        P("kv", "tp", None),
        P("kv", "tp"),
        P(None, "tp"),
        P("tp"),
        P("tp", "kv"),
        P("tp", "kv"),
        P("kv", "tp"),
    )
    return jax.shard_map(
        make(mesh.shape["kv"], mesh.shape["tp"]),
        mesh=mesh,
        in_specs=placed,
        out_specs=(P("kv", "tp"), P("kv", "tp", None, None), P("kv", "tp", None), P("kv", "tp")),
        check_vma=False,
    )
```

```python
import functools

import jax
import jax.numpy as jnp
from jax import lax
from jax.experimental import pallas as pl
from jax.experimental.pallas import tpu as pltpu
from jax.sharding import PartitionSpec as P

BF16 = jnp.bfloat16
F32 = jnp.float32
LANES = 128
COVER = 2**36
HBM = pl.BlockSpec(memory_space=pltpu.HBM)
VMEM = pl.BlockSpec(memory_space=pltpu.VMEM)
NT = (((1,), (1,)), ((), ()))


def shifted(x, axis, size, step):
    return lax.ppermute(x, axis, [(i, (i + step) % size) for i in range(size)])


def partner(i, step, size):
    return i ^ step if size & (size - 1) == 0 else (i + step) % size


def group_sizes(size):
    low = 1
    while low * low < size:
        low *= 2
    return (size // low, low) if size % low == 0 else (size, 1)


def exchange(x, axis, size, low, step, inner):
    pairs = []
    for k in range(size):
        a, b = divmod(k, low)
        b2 = partner(b, step, low) if inner else b
        a2 = a if inner else partner(a, step, size // low)
        pairs.append((k, a2 * low + b2))
    return lax.ppermute(x, axis, pairs)


def column_pieces(x, axis, size):
    if size != 2:
        return [lax.all_gather(x, axis, axis=1, tiled=True)]
    return [x, shifted(x, axis, size, 1)]


def in_vmem(x):
    return pltpu.with_memory_space_constraint(x, pltpu.VMEM)


def in_hbm(x):
    return pltpu.with_memory_space_constraint(x, pltpu.HBM)


def piece_starts(refs, axis):
    if len(refs) == 1:
        return [0]
    me, width = lax.axis_index(axis), refs[0].shape[1]
    return [pl.multiple_of(me * width, LANES), pl.multiple_of((1 - me) * width, LANES)]


def load_kernel(count, *refs):
    sources, targets, sem = refs[:count], refs[count : 2 * count], refs[-1]
    copies = [pltpu.make_async_copy(a, b, sem.at[i]) for i, (a, b) in enumerate(zip(sources, targets))]
    for copy in copies:
        copy.start()
    for copy in copies:
        copy.wait()


def load(arrays):
    return pl.pallas_call(
        functools.partial(load_kernel, len(arrays)),
        name="load",
        out_shape=[pltpu.VMEM(x.shape, x.dtype) for x in arrays],
        in_specs=[HBM] * len(arrays),
        out_specs=[VMEM] * len(arrays),
        scratch_shapes=[pltpu.SemaphoreType.DMA((len(arrays),))],
        compiler_params=pltpu.CompilerParams(vmem_limit_bytes=4 * 2**20),
        cost_estimate=pl.CostEstimate(flops=COVER, bytes_accessed=2**18, transcendentals=0),
    )(*map(in_hbm, arrays))


def read_kernel(pieces, *refs):
    token_refs, refs = refs[:pieces], refs[pieces:]
    (gain, wi, wf, old_max_t, wq, memory, *refs) = refs
    (normed_out, query_out, old_part, keep_out, admit_out, floor_out, new_max_t, full) = refs
    rows, heads, dim = memory.shape[:3]

    for ref, start in zip(token_refs, piece_starts(token_refs, "tp")):
        full[:, pl.ds(start, ref.shape[1])] = ref[...].astype(F32)
    x = full[...]
    scale = lax.rsqrt(jnp.mean(x * x, axis=1, keepdims=True) + 1e-06)
    normed = (x * scale * gain[...]).astype(BF16)
    normed_out[...] = normed

    def nt(a, b):
        return lax.dot_general(a, b, NT, preferred_element_type=F32)

    all_heads = wi.shape[0]
    me = lax.axis_index("tp")

    def own_heads(x):
        out = x[:heads]
        for i in range(1, all_heads // heads):
            out = jnp.where(me == i, x[i * heads : (i + 1) * heads], out)
        return out

    queries = jnp.dot(normed, wq[...], preferred_element_type=F32) * dim ** (-0.5)
    query_out[...] = queries
    igate = own_heads(nt(wi[...], normed))
    lforget = jax.nn.log_sigmoid(own_heads(nt(wf[...], normed)))
    old_max = old_max_t[...]
    max_t = jnp.maximum(lforget + old_max, igate)
    new_max_t[...] = max_t
    keep_out[...] = jnp.exp(lforget + old_max - max_t).T
    admit_out[...] = jnp.exp(igate - max_t).T
    floor_out[...] = jnp.exp(-max_t).T

    columns = [queries[:, h * dim : (h + 1) * dim].T for h in range(heads)]
    for b in range(rows):
        for h in range(heads):
            part = jnp.sum(memory[b, h] * columns[h][:, b : b + 1], axis=0, keepdims=True)
            old_part[h, b : b + 1, :] = part


def run_read(token_pieces, gain, wi, wf, old_max_t, wq, memory):
    rows, heads, dim = memory.shape[:3]
    depth, inner = wq.shape
    flops = 2 * rows * depth * inner
    return pl.pallas_call(
        functools.partial(read_kernel, len(token_pieces)),
        name="read",
        out_shape=[
            pltpu.VMEM((rows, depth), BF16),
            pltpu.VMEM((rows, inner), F32),
            pltpu.VMEM((heads, rows, dim), F32),
            pltpu.VMEM((rows, heads), F32),
            pltpu.VMEM((rows, heads), F32),
            pltpu.VMEM((rows, heads), F32),
            jax.ShapeDtypeStruct((heads, rows), F32),
        ],
        in_specs=[VMEM] * (len(token_pieces) + 6),
        out_specs=[VMEM] * 7,
        scratch_shapes=[pltpu.VMEM((rows, depth), F32)],
        compiler_params=pltpu.CompilerParams(vmem_limit_bytes=16 * 2**20),
        cost_estimate=pl.CostEstimate(flops=flops * 32, bytes_accessed=6 * 2**20, transcendentals=0),
    )(*token_pieces, gain, wi, wf, old_max_t, *map(in_vmem, [wq, memory]))


def mix_kernel(*refs):
    (normed, query, old_part, keep, admit, floor, normalizer, wk, wv, wo, *refs) = refs
    (mixed, new_normalizer, key_out, value_out) = refs
    rows, heads, dim = normalizer.shape

    def head(x, h):
        return x[:, h * dim : (h + 1) * dim]

    x = normed[...]
    keys = jnp.dot(x, wk[...], preferred_element_type=F32)
    values = jnp.dot(x, wv[...], preferred_element_type=F32)
    outgate = jax.nn.sigmoid(jnp.dot(x, wo[...], preferred_element_type=F32))
    key_out[...] = keys
    value_out[...] = values
    for h in range(heads):
        q, k, v = head(query[...], h), head(keys, h), head(values, h)
        kw, aw = keep[:, h : h + 1], admit[:, h : h + 1]
        norm = kw * normalizer[:, h, :] + aw * k
        new_normalizer[:, h, :] = norm
        query_key = jnp.sum(q * k, axis=1, keepdims=True)
        denominator = jnp.sum(q * norm, axis=1, keepdims=True)
        numerator = kw * old_part[h] + (aw * query_key) * v
        cell_out = numerator / jnp.maximum(jnp.abs(denominator), floor[:, h : h + 1])
        centered = cell_out - jnp.mean(cell_out, axis=1, keepdims=True)
        variance = jnp.mean(centered * centered, axis=1, keepdims=True)
        gated = head(outgate, h) * centered * lax.rsqrt(variance + 1e-05)
        mixed[:, h * dim : (h + 1) * dim] = gated.astype(BF16)


def run_mix(normed, query, old_part, keep, admit, floor, normalizer, weights):
    rows, heads, dim = normalizer.shape
    depth, inner = weights[0].shape
    flops = 2 * rows * depth * inner * len(weights)
    return pl.pallas_call(
        mix_kernel,
        name="mix",
        out_shape=[
            pltpu.VMEM((rows, inner), BF16),
            jax.ShapeDtypeStruct((rows, heads, dim), F32),
            pltpu.VMEM((rows, inner), F32),
            pltpu.VMEM((rows, inner), F32),
        ],
        in_specs=[VMEM] * 10,
        out_specs=[VMEM] * 4,
        compiler_params=pltpu.CompilerParams(vmem_limit_bytes=16 * 2**20),
        cost_estimate=pl.CostEstimate(flops=flops * 32, bytes_accessed=6 * 2**20, transcendentals=0),
    )(normed, query, old_part, keep, admit, floor, normalizer, *map(in_vmem, weights))


def out_kernel(pieces, *refs):
    mixed_refs, (tokens, w_output, resid) = refs[:pieces], refs[pieces:]
    total = tokens[...].astype(F32)
    for ref, start in zip(mixed_refs, piece_starts(mixed_refs, "tp")):
        weight = w_output[pl.ds(start, ref.shape[1]), :]
        total = total + jnp.dot(ref[...], weight, preferred_element_type=F32)
    resid[...] = total.astype(BF16)


def run_out(mixed_pieces, tokens, w_output):
    rows, width = tokens.shape
    return pl.pallas_call(
        functools.partial(out_kernel, len(mixed_pieces)),
        name="out_projection",
        out_shape=pltpu.VMEM((rows, width), BF16),
        in_specs=[VMEM] * (len(mixed_pieces) + 2),
        out_specs=VMEM,
        compiler_params=pltpu.CompilerParams(vmem_limit_bytes=24 * 2**20),
        cost_estimate=pl.CostEstimate(
            flops=2 * rows * w_output.size, bytes_accessed=2 * w_output.size, transcendentals=0
        ),
    )(*mixed_pieces, tokens, w_output)


def stack_kernel(low, *refs):
    *pieces, out = refs
    me = lax.div(lax.axis_index("kv"), low)
    for step, ref in enumerate(pieces):
        out[partner(me, step, out.shape[0])] = ref[...]


def run_stack(pieces, low):
    return pl.pallas_call(
        functools.partial(stack_kernel, low),
        name="stack",
        out_shape=pltpu.VMEM((len(pieces), *pieces[0].shape), BF16),
        in_specs=[VMEM] * len(pieces),
        out_specs=VMEM,
        compiler_params=pltpu.CompilerParams(vmem_limit_bytes=16 * 2**20),
        cost_estimate=pl.CostEstimate(flops=2**20, bytes_accessed=2**18, transcendentals=0),
    )(*pieces)


def up_kernel(pieces, *refs):
    piece_refs, (gain, w_gate, w_up, own, sent) = refs[:pieces], refs[pieces:]
    hidden = w_gate.shape[0]
    half = own.shape[1] // 2
    x = jnp.concatenate([ref[...].reshape(-1, ref.shape[2]) for ref in piece_refs], axis=0).astype(F32)
    squares = jnp.sum(x * x, axis=1, keepdims=True)
    ffn_in = (x * gain[...]).astype(BF16)
    own[...] = jnp.zeros_like(own)
    for weight, first in [(w_gate, 0), (w_up, half)]:
        own[:, first : first + hidden] = lax.dot_general(ffn_in, weight[...], NT, preferred_element_type=F32)
    lane = lax.broadcasted_iota(jnp.int32, (x.shape[0], LANES), 1)
    high = squares.astype(BF16).astype(F32)
    first = hidden // LANES * LANES
    tile = own[:, first : first + LANES]
    spot = hidden - first
    own[:, first : first + LANES] = jnp.where(lane == spot, squares, tile)
    sent[...] = own[...].astype(BF16)
    tile = jnp.where(lane == spot, high, jnp.where(lane == spot + 1, squares - high, tile))
    sent[:, first : first + LANES] = tile.astype(BF16)


def run_up(pieces, gain, w_gate, w_up):
    rows, depth = sum(x.shape[0] * x.shape[1] for x in pieces), pieces[0].shape[2]
    hidden = w_gate.shape[1]
    half = (hidden + 2 + LANES - 1) // LANES * LANES
    return pl.pallas_call(
        functools.partial(up_kernel, len(pieces)),
        name="gate_up",
        out_shape=[jax.ShapeDtypeStruct((rows, 2 * half), F32), jax.ShapeDtypeStruct((rows, 2 * half), BF16)],
        in_specs=[VMEM] * (len(pieces) + 3),
        out_specs=[VMEM, VMEM],
        compiler_params=pltpu.CompilerParams(vmem_limit_bytes=24 * 2**20),
        cost_estimate=pl.CostEstimate(flops=4 * rows * depth * hidden, bytes_accessed=4 * 2**20, transcendentals=0),
    )(*pieces, gain, w_gate.T, w_up.T)


def down_kernel(others, channels, low, own, *refs):
    other_refs, (w_down, *refs) = refs[:others], refs[others:]
    kept, *sent = refs
    hidden = w_down.shape[0]
    half = own.shape[1] // 2
    gate, up = own[:, :half], own[:, half:]
    squares = gate[:, hidden : hidden + 1]
    for ref in other_refs:
        theirs = ref[...].astype(F32)
        gate, up = gate + theirs[:, :half], up + theirs[:, half:]
        squares = squares + theirs[:, hidden : hidden + 1] + theirs[:, hidden + 1 : hidden + 2]
    scale = lax.rsqrt(squares / channels + 1e-06)
    gate = scale * gate[:, :hidden]
    act = (gate * jax.nn.sigmoid(gate) * (scale * up[:, :hidden])).astype(BF16)
    full = jnp.dot(act, w_down[...], preferred_element_type=F32).reshape(low, *kept.shape)
    kept[...] = full[0]
    for step, ref in enumerate(sent, 1):
        ref[...] = full[step].astype(BF16)


def run_down(own, others, w_down, channels, high, low):
    rows = own.shape[0] // (high * low)
    hidden, width = w_down.shape
    return pl.pallas_call(
        functools.partial(down_kernel, len(others), channels, low),
        name="down",
        out_shape=[pltpu.VMEM((high, rows, width), F32)] + [pltpu.VMEM((high, rows, width), BF16)] * (low - 1),
        in_specs=[VMEM] * (2 + len(others)),
        out_specs=[VMEM] * low,
        compiler_params=pltpu.CompilerParams(vmem_limit_bytes=24 * 2**20),
        cost_estimate=pl.CostEstimate(flops=2 * own.shape[0] * width * hidden, bytes_accessed=2**21, transcendentals=0),
    )(own, *others, w_down)


def fold_kernel(count, low, kept, *refs):
    received, (own, *sent), total = refs[:count], refs[count:-1], refs[-1]
    x = kept[...]
    for ref in received:
        x = x + ref[...].astype(F32)
    total[...] = x
    high = kept.shape[0]
    me = lax.div(lax.axis_index("kv"), low)
    own[...] = total[me]
    for step, ref in enumerate(sent, 1):
        ref[...] = total[partner(me, step, high)].astype(BF16)


def run_fold(kept, received, low):
    high, rows, width = kept.shape
    return pl.pallas_call(
        functools.partial(fold_kernel, len(received), low),
        name="fold",
        out_shape=[pltpu.VMEM((rows, width), F32)] + [pltpu.VMEM((rows, width), BF16)] * (high - 1),
        in_specs=[VMEM] * (1 + len(received)),
        out_specs=[VMEM] * high,
        scratch_shapes=[pltpu.VMEM(kept.shape, F32)],
        compiler_params=pltpu.CompilerParams(vmem_limit_bytes=16 * 2**20),
        cost_estimate=pl.CostEstimate(flops=2**24, bytes_accessed=2**20, transcendentals=0),
    )(kept, *received)


def make(kv, tp):
    def per_device(
        tokens,
        norm_gain,
        w_query,
        w_key,
        w_value,
        w_outgate,
        w_input_gate,
        w_forget_gate,
        memory,
        normalizer,
        memory_max,
        w_output,
        ffn_gain,
        w_gate,
        w_up,
        w_down,
    ):
        rows, own_channels = tokens.shape
        heads, head_dim = memory.shape[1], memory.shape[2]
        own, gain, wi, wf, old_normalizer, old_max_t = load(
            [tokens, norm_gain[None], w_input_gate.T, w_forget_gate.T, normalizer, memory_max.T]
        )
        pieces = column_pieces(own, "tp", tp)
        normed, query, old_part, keep, admit, floor, new_max_t = run_read(
            pieces, gain, wi, wf, old_max_t, w_query, memory
        )
        mixed, new_normalizer, keys, values = run_mix(
            normed, query, old_part, keep, admit, floor, old_normalizer, [w_key, w_value, w_outgate]
        )
        pieces = column_pieces(mixed, "tp", tp)
        resid = run_out(pieces, tokens, w_output)
        high, low = group_sizes(kv)
        column = [resid] + [exchange(resid, "kv", kv, low, step, False) for step in range(1, high)]
        block = run_stack(column, low)
        every_row = [block] + [exchange(block, "kv", kv, low, step, True) for step in range(1, low)]
        by_head = (rows, heads, head_dim)
        keys, values = keys.reshape(by_head), values.reshape(by_head)
        new_memory = keep[..., None, None] * memory + admit[..., None, None] * (
            keys[..., :, None] * values[..., None, :]
        )

        own, sent = run_up(every_row, ffn_gain[None], w_gate, w_up)
        others = [shifted(sent, "tp", tp, step) for step in range(1, tp)]
        kept, *sent = run_down(own, others, w_down, own_channels * tp, high, low)
        received = [exchange(x, "kv", kv, low, step, True) for step, x in enumerate(sent, 1)]
        *received, new_memory = lax.optimization_barrier((*received, new_memory))
        kept, *sent = run_fold(kept, received, low)
        received = [exchange(x, "kv", kv, low, step, False) for step, x in enumerate(sent, 1)]
        down_out = kept
        for x in received:
            down_out = down_out + x.astype(F32)
        result = (resid.astype(F32) + down_out).astype(BF16)
        return (result, new_memory, new_normalizer, new_max_t.T)

    return per_device


def solution(mesh):
    placed = (
        P("kv", "tp"),
        P(),
        P(None, "tp"),
        P(None, "tp"),
        P(None, "tp"),
        P(None, "tp"),
        P(),
        P(),
        P("kv", "tp", None, None),
        P("kv", "tp", None),
        P("kv", "tp"),
        P(None, "tp"),
        P("tp"),
        P("tp", "kv"),
        P("tp", "kv"),
        P("kv", "tp"),
    )
    return jax.shard_map(
        make(mesh.shape["kv"], mesh.shape["tp"]),
        mesh=mesh,
        in_specs=placed,
        out_specs=(P("kv", "tp"), P("kv", "tp", None, None), P("kv", "tp", None), P("kv", "tp")),
        check_vma=False,
    )
```

```python
import functools

import jax
import jax.numpy as jnp
from jax import lax
from jax.experimental import pallas as pl
from jax.experimental.pallas import tpu as pltpu
from jax.sharding import PartitionSpec as P


BF16 = jnp.bfloat16
F32 = jnp.float32
LANES = 128
COVER = 2**36
HBM = pl.BlockSpec(memory_space=pltpu.HBM)
VMEM = pl.BlockSpec(memory_space=pltpu.VMEM)
NT = (((1,), (1,)), ((), ()))


def shifted(x, axis, size, step):
    return lax.ppermute(x, axis, [(i, (i + step) % size) for i in range(size)])


def partner(i, step, size):
    return i ^ step if size & (size - 1) == 0 else (i + step) % size


def group_sizes(size):
    low = 1
    while low * low < size:
        low *= 2
    return (size // low, low) if size % low == 0 else (size, 1)


def exchange(x, axis, size, low, step, inner):
    pairs = []
    for k in range(size):
        a, b = divmod(k, low)
        b2 = partner(b, step, low) if inner else b
        a2 = a if inner else partner(a, step, size // low)
        pairs.append((k, a2 * low + b2))
    return lax.ppermute(x, axis, pairs)


def staged(sent, size, low, inner):
    received = []
    for step, x in enumerate(sent, 1):
        received.append(exchange(x, "kv", size, low, step, inner))
    return received


def column_pieces(x, axis, size):
    if size != 2:
        return [lax.all_gather(x, axis, axis=1, tiled=True)]
    return [x, shifted(x, axis, size, 1)]


def in_vmem(x):
    return pltpu.with_memory_space_constraint(x, pltpu.VMEM)


def in_hbm(x):
    return pltpu.with_memory_space_constraint(x, pltpu.HBM)


def piece_starts(refs, axis):
    if len(refs) == 1:
        return [0]
    me, width = lax.axis_index(axis), refs[0].shape[1]
    return [pl.multiple_of(me * width, LANES), pl.multiple_of((1 - me) * width, LANES)]


def load_kernel(count, *refs):
    sources, targets, sem = refs[:count], refs[count : 2 * count], refs[-1]
    copies = [pltpu.make_async_copy(a, b, sem.at[i]) for i, (a, b) in enumerate(zip(sources, targets))]
    for copy in copies:
        copy.start()
    for copy in copies:
        copy.wait()


def load(arrays):
    return pl.pallas_call(
        functools.partial(load_kernel, len(arrays)),
        name="load",
        out_shape=[pltpu.VMEM(x.shape, x.dtype) for x in arrays],
        in_specs=[HBM] * len(arrays),
        out_specs=[VMEM] * len(arrays),
        scratch_shapes=[pltpu.SemaphoreType.DMA((len(arrays),))],
        compiler_params=pltpu.CompilerParams(vmem_limit_bytes=4 * 2**20),
        cost_estimate=pl.CostEstimate(flops=COVER, bytes_accessed=2**18, transcendentals=0),
    )(*map(in_hbm, arrays))


def read_kernel(pieces, *refs):
    token_refs, refs = refs[:pieces], refs[pieces:]
    (gain, wi, wf, old_max_t, wq, memory, *refs) = refs
    (normed_out, query_out, old_part, keep_out, admit_out, floor_out, new_max_t, full) = refs
    rows, heads, dim = memory.shape[:3]

    for ref, start in zip(token_refs, piece_starts(token_refs, "tp")):
        full[:, pl.ds(start, ref.shape[1])] = ref[...].astype(F32)
    x = full[...]
    scale = lax.rsqrt(jnp.mean(x * x, axis=1, keepdims=True) + 1e-06)
    normed = (x * scale * gain[...]).astype(BF16)
    normed_out[...] = normed

    def nt(a, b):
        return lax.dot_general(a, b, NT, preferred_element_type=F32)

    all_heads = wi.shape[0]
    me = lax.axis_index("tp")

    def own_heads(x):
        out = x[:heads]
        for i in range(1, all_heads // heads):
            out = jnp.where(me == i, x[i * heads : (i + 1) * heads], out)
        return out

    queries = jnp.dot(normed, wq[...], preferred_element_type=F32) * dim ** (-0.5)
    query_out[...] = queries
    igate = own_heads(nt(wi[...], normed))
    lforget = jax.nn.log_sigmoid(own_heads(nt(wf[...], normed)))
    old_max = old_max_t[...]
    max_t = jnp.maximum(lforget + old_max, igate)
    new_max_t[...] = max_t
    keep_out[...] = jnp.exp(lforget + old_max - max_t).T
    admit_out[...] = jnp.exp(igate - max_t).T
    floor_out[...] = jnp.exp(-max_t).T

    columns = [queries[:, h * dim : (h + 1) * dim].T for h in range(heads)]
    for b in range(rows):
        for h in range(heads):
            part = jnp.sum(memory[b, h] * columns[h][:, b : b + 1], axis=0, keepdims=True)
            old_part[h, b : b + 1, :] = part


def run_read(token_pieces, gain, wi, wf, old_max_t, wq, memory):
    rows, heads, dim = memory.shape[:3]
    depth, inner = wq.shape
    return pl.pallas_call(
        functools.partial(read_kernel, len(token_pieces)),
        name="read",
        out_shape=[
            pltpu.VMEM((rows, depth), BF16),
            pltpu.VMEM((rows, inner), F32),
            pltpu.VMEM((heads, rows, dim), F32),
            pltpu.VMEM((rows, heads), F32),
            pltpu.VMEM((rows, heads), F32),
            pltpu.VMEM((rows, heads), F32),
            jax.ShapeDtypeStruct((heads, rows), F32),
        ],
        in_specs=[VMEM] * (len(token_pieces) + 6),
        out_specs=[VMEM] * 7,
        scratch_shapes=[pltpu.VMEM((rows, depth), F32)],
        compiler_params=pltpu.CompilerParams(vmem_limit_bytes=16 * 2**20),
        cost_estimate=pl.CostEstimate(flops=2**30, bytes_accessed=6 * 2**20, transcendentals=0),
    )(*token_pieces, gain, wi, wf, old_max_t, *map(in_vmem, [wq, memory]))


def mix_kernel(*refs):
    (normed, query, old_part, keep, admit, floor, normalizer, wk, wv, wo, *refs) = refs
    (mixed, new_normalizer, key_out, value_out) = refs
    _, heads, dim = normalizer.shape

    def head(x, h):
        return x[:, h * dim : (h + 1) * dim]

    x = normed[...]
    keys = jnp.dot(x, wk[...], preferred_element_type=F32)
    values = jnp.dot(x, wv[...], preferred_element_type=F32)
    outgate = jax.nn.sigmoid(jnp.dot(x, wo[...], preferred_element_type=F32))
    key_out[...] = keys
    value_out[...] = values
    for h in range(heads):
        q, k, v = head(query[...], h), head(keys, h), head(values, h)
        kw, aw = keep[:, h : h + 1], admit[:, h : h + 1]
        norm = kw * normalizer[:, h, :] + aw * k
        new_normalizer[:, h, :] = norm
        query_key = jnp.sum(q * k, axis=1, keepdims=True)
        denominator = jnp.sum(q * norm, axis=1, keepdims=True)
        numerator = kw * old_part[h] + (aw * query_key) * v
        cell_out = numerator / jnp.maximum(jnp.abs(denominator), floor[:, h : h + 1])
        centered = cell_out - jnp.mean(cell_out, axis=1, keepdims=True)
        variance = jnp.mean(centered * centered, axis=1, keepdims=True)
        gated = head(outgate, h) * centered * lax.rsqrt(variance + 1e-05)
        mixed[:, h * dim : (h + 1) * dim] = gated.astype(BF16)


def run_mix(normed, query, old_part, keep, admit, floor, normalizer, weights):
    rows, heads, dim = normalizer.shape
    depth, inner = weights[0].shape
    flops = 2 * rows * depth * inner * len(weights)
    return pl.pallas_call(
        mix_kernel,
        name="mix",
        out_shape=[
            pltpu.VMEM((rows, inner), BF16),
            jax.ShapeDtypeStruct((rows, heads, dim), F32),
            pltpu.VMEM((rows, inner), F32),
            pltpu.VMEM((rows, inner), F32),
        ],
        in_specs=[VMEM] * 10,
        out_specs=[VMEM] * 4,
        compiler_params=pltpu.CompilerParams(vmem_limit_bytes=16 * 2**20),
        cost_estimate=pl.CostEstimate(flops=flops * 32, bytes_accessed=6 * 2**20, transcendentals=0),
    )(normed, query, old_part, keep, admit, floor, normalizer, *map(in_vmem, weights))


def out_kernel(pieces, *refs):
    mixed_refs, (tokens, w_output, resid) = refs[:pieces], refs[pieces:]
    total = tokens[...].astype(F32)
    for ref, start in zip(mixed_refs, piece_starts(mixed_refs, "tp")):
        weight = w_output[pl.ds(start, ref.shape[1]), :]
        total = total + jnp.dot(ref[...], weight, preferred_element_type=F32)
    resid[...] = total.astype(BF16)


def run_out(mixed_pieces, tokens, w_output):
    rows, width = tokens.shape
    return pl.pallas_call(
        functools.partial(out_kernel, len(mixed_pieces)),
        name="out_projection",
        out_shape=pltpu.VMEM((rows, width), BF16),
        in_specs=[VMEM] * (len(mixed_pieces) + 2),
        out_specs=VMEM,
        compiler_params=pltpu.CompilerParams(vmem_limit_bytes=24 * 2**20),
        cost_estimate=pl.CostEstimate(
            flops=2 * rows * w_output.size, bytes_accessed=2 * w_output.size, transcendentals=0
        ),
    )(*mixed_pieces, tokens, w_output)


def stack_kernel(low, *refs):
    *pieces, out = refs
    me = lax.div(lax.axis_index("kv"), low)
    for step, ref in enumerate(pieces):
        out[partner(me, step, out.shape[0])] = ref[...]


def run_stack(pieces, low):
    return pl.pallas_call(
        functools.partial(stack_kernel, low),
        name="stack",
        out_shape=pltpu.VMEM((len(pieces), *pieces[0].shape), BF16),
        in_specs=[VMEM] * len(pieces),
        out_specs=VMEM,
        compiler_params=pltpu.CompilerParams(vmem_limit_bytes=16 * 2**20),
        cost_estimate=pl.CostEstimate(flops=2**20, bytes_accessed=2**18, transcendentals=0),
    )(*pieces)


def up_kernel(pieces, *refs):
    piece_refs, (gain, w_gate, w_up, own, sent) = refs[:pieces], refs[pieces:]
    hidden = w_gate.shape[0]
    half = own.shape[1] // 2
    x = jnp.concatenate([ref[...].reshape(-1, ref.shape[2]) for ref in piece_refs], axis=0).astype(F32)
    squares = jnp.sum(x * x, axis=1, keepdims=True)
    ffn_in = (x * gain[...]).astype(BF16)
    own[...] = jnp.zeros_like(own)
    for weight, first in [(w_gate, 0), (w_up, half)]:
        own[:, first : first + hidden] = lax.dot_general(ffn_in, weight[...], NT, preferred_element_type=F32)
    lane = lax.broadcasted_iota(jnp.int32, (x.shape[0], LANES), 1)
    high = squares.astype(BF16).astype(F32)
    first = hidden // LANES * LANES
    tile = own[:, first : first + LANES]
    spot = hidden - first
    own[:, first : first + LANES] = jnp.where(lane == spot, squares, tile)
    sent[...] = own[...].astype(BF16)
    tile = jnp.where(lane == spot, high, jnp.where(lane == spot + 1, squares - high, tile))
    sent[:, first : first + LANES] = tile.astype(BF16)


def run_up(pieces, gain, w_gate, w_up):
    rows, depth = sum(x.shape[0] * x.shape[1] for x in pieces), pieces[0].shape[2]
    hidden = w_gate.shape[1]
    half = (hidden + 2 + LANES - 1) // LANES * LANES
    return pl.pallas_call(
        functools.partial(up_kernel, len(pieces)),
        name="gate_up",
        out_shape=[jax.ShapeDtypeStruct((rows, 2 * half), F32), jax.ShapeDtypeStruct((rows, 2 * half), BF16)],
        in_specs=[VMEM] * (len(pieces) + 3),
        out_specs=[VMEM, VMEM],
        compiler_params=pltpu.CompilerParams(vmem_limit_bytes=24 * 2**20),
        cost_estimate=pl.CostEstimate(flops=4 * rows * depth * hidden, bytes_accessed=4 * 2**20, transcendentals=0),
    )(*pieces, gain, w_gate.T, w_up.T)


def down_kernel(others, channels, low, own, *refs):
    other_refs, (w_down, *refs) = refs[:others], refs[others:]
    kept, *sent = refs
    hidden = w_down.shape[0]
    half = own.shape[1] // 2
    gate, up = own[:, :half], own[:, half:]
    squares = gate[:, hidden : hidden + 1]
    for ref in other_refs:
        theirs = ref[...].astype(F32)
        gate, up = gate + theirs[:, :half], up + theirs[:, half:]
        squares = squares + theirs[:, hidden : hidden + 1] + theirs[:, hidden + 1 : hidden + 2]
    scale = lax.rsqrt(squares / channels + 1e-06)
    gate = scale * gate[:, :hidden]
    act = (gate * jax.nn.sigmoid(gate) * (scale * up[:, :hidden])).astype(BF16)
    full = jnp.dot(act, w_down[...], preferred_element_type=F32).reshape(low, *kept.shape)
    kept[...] = full[0]
    for step, ref in enumerate(sent, 1):
        ref[...] = full[step].astype(BF16)


def run_down(own, others, w_down, channels, high, low):
    rows = own.shape[0] // (high * low)
    hidden, width = w_down.shape
    return pl.pallas_call(
        functools.partial(down_kernel, len(others), channels, low),
        name="down",
        out_shape=[pltpu.VMEM((high, rows, width), F32)] + [pltpu.VMEM((high, rows, width), BF16)] * (low - 1),
        in_specs=[VMEM] * (2 + len(others)),
        out_specs=[VMEM] * low,
        compiler_params=pltpu.CompilerParams(vmem_limit_bytes=24 * 2**20),
        cost_estimate=pl.CostEstimate(flops=2 * own.shape[0] * width * hidden, bytes_accessed=2**21, transcendentals=0),
    )(own, *others, w_down)


def fold_kernel(count, low, kept, *refs):
    received, (own, *sent), total = refs[:count], refs[count:-1], refs[-1]
    x = kept[...]
    for ref in received:
        x = x + ref[...].astype(F32)
    total[...] = x
    high = kept.shape[0]
    me = lax.div(lax.axis_index("kv"), low)
    own[...] = total[me]
    for step, ref in enumerate(sent, 1):
        ref[...] = total[partner(me, step, high)].astype(BF16)


def run_fold(kept, received, low):
    high, rows, width = kept.shape
    return pl.pallas_call(
        functools.partial(fold_kernel, len(received), low),
        name="fold",
        out_shape=[pltpu.VMEM((rows, width), F32)] + [pltpu.VMEM((rows, width), BF16)] * (high - 1),
        in_specs=[VMEM] * (1 + len(received)),
        out_specs=[VMEM] * high,
        scratch_shapes=[pltpu.VMEM(kept.shape, F32)],
        compiler_params=pltpu.CompilerParams(vmem_limit_bytes=16 * 2**20),
        cost_estimate=pl.CostEstimate(flops=2**24, bytes_accessed=2**20, transcendentals=0),
    )(kept, *received)


def make(kv, tp):
    def per_device(
        tokens,
        norm_gain,
        w_query,
        w_key,
        w_value,
        w_outgate,
        w_input_gate,
        w_forget_gate,
        memory,
        normalizer,
        memory_max,
        w_output,
        ffn_gain,
        w_gate,
        w_up,
        w_down,
    ):
        rows, own_channels = tokens.shape
        heads, head_dim = memory.shape[1], memory.shape[2]
        own, gain, wi, wf, old_normalizer, old_max_t = load(
            [tokens, norm_gain[None], w_input_gate.T, w_forget_gate.T, normalizer, memory_max.T]
        )
        pieces = column_pieces(own, "tp", tp)
        normed, query, old_part, keep, admit, floor, new_max_t = run_read(
            pieces, gain, wi, wf, old_max_t, w_query, memory
        )
        mixed, new_normalizer, keys, values = run_mix(
            normed, query, old_part, keep, admit, floor, old_normalizer, [w_key, w_value, w_outgate]
        )
        pieces = column_pieces(mixed, "tp", tp)
        resid = run_out(pieces, tokens, w_output)
        high, low = group_sizes(kv)
        column = [resid] + staged([resid] * (high - 1), kv, low, False)
        block = run_stack(column, low)
        every_row = [block] + staged([block] * (low - 1), kv, low, True)
        by_head = (rows, heads, head_dim)
        outer = keys.reshape(by_head)[..., :, None] * values.reshape(by_head)[..., None, :]
        new_memory = keep[..., None, None] * memory + admit[..., None, None] * outer
        own, sent = run_up(every_row, ffn_gain[None], w_gate, w_up)
        others = [shifted(sent, "tp", tp, step) for step in range(1, tp)]
        kept, *sent = run_down(own, others, w_down, own_channels * tp, high, low)
        received = staged(sent, kv, low, True)
        kept, *sent = run_fold(kept, received, low)
        received = staged(sent, kv, low, False)
        down_out = kept
        for x in received:
            down_out = down_out + x.astype(F32)
        result = (resid.astype(F32) + down_out).astype(BF16)
        return (result, new_memory, new_normalizer, new_max_t.T)

    return per_device


def solution(mesh):
    placed = (
        P("kv", "tp"),
        P(),
        P(None, "tp"),
        P(None, "tp"),
        P(None, "tp"),
        P(None, "tp"),
        P(),
        P(),
        P("kv", "tp", None, None),
        P("kv", "tp", None),
        P("kv", "tp"),
        P(None, "tp"),
        P("tp"),
        P("tp", "kv"),
        P("tp", "kv"),
        P("kv", "tp"),
    )
    body = make(mesh.shape["kv"], mesh.shape["tp"])

    return jax.shard_map(
        body,
        mesh=mesh,
        in_specs=placed,
        out_specs=(P("kv", "tp"), P("kv", "tp", None, None), P("kv", "tp", None), P("kv", "tp")),
        check_vma=False,
    )
```

```python
import functools

import jax
import jax.numpy as jnp
from jax import lax
from jax.experimental import pallas as pl
from jax.experimental.pallas import tpu as pltpu
from jax.sharding import PartitionSpec as P


BF16 = jnp.bfloat16
F32 = jnp.float32
LANES = 128
COVER = 2**36
HBM = pl.BlockSpec(memory_space=pltpu.HBM)
VMEM = pl.BlockSpec(memory_space=pltpu.VMEM)
NT = (((1,), (1,)), ((), ()))


def shifted(x, axis, size, step):
    return lax.ppermute(x, axis, [(i, (i + step) % size) for i in range(size)])


def partner(i, step, size):
    return i ^ step if size & (size - 1) == 0 else (i + step) % size


def group_sizes(size):
    low = 1
    while low * low < size:
        low *= 2
    return (size // low, low) if size % low == 0 else (size, 1)


def exchange(x, axis, size, low, step, inner):
    pairs = []
    for k in range(size):
        a, b = divmod(k, low)
        b2 = partner(b, step, low) if inner else b
        a2 = a if inner else partner(a, step, size // low)
        pairs.append((k, a2 * low + b2))
    return lax.ppermute(x, axis, pairs)


def staged(sent, size, low, inner):
    received = []
    for step, x in enumerate(sent, 1):
        received.append(exchange(x, "kv", size, low, step, inner))
    return received


def column_pieces(x, axis, size):
    if size != 2:
        return [lax.all_gather(x, axis, axis=1, tiled=True)]
    return [x, shifted(x, axis, size, 1)]


def in_vmem(x):
    return pltpu.with_memory_space_constraint(x, pltpu.VMEM)


def in_hbm(x):
    return pltpu.with_memory_space_constraint(x, pltpu.HBM)


def piece_starts(refs, axis):
    if len(refs) == 1:
        return [0]
    me, width = lax.axis_index(axis), refs[0].shape[1]
    return [pl.multiple_of(me * width, LANES), pl.multiple_of((1 - me) * width, LANES)]


def load_kernel(count, *refs):
    sources, targets, sem = refs[:count], refs[count : 2 * count], refs[-1]
    copies = [pltpu.make_async_copy(a, b, sem.at[i]) for i, (a, b) in enumerate(zip(sources, targets))]
    for copy in copies:
        copy.start()
    for copy in copies:
        copy.wait()


def load(arrays):
    return pl.pallas_call(
        functools.partial(load_kernel, len(arrays)),
        name="load",
        out_shape=[pltpu.VMEM(x.shape, x.dtype) for x in arrays],
        in_specs=[HBM] * len(arrays),
        out_specs=[VMEM] * len(arrays),
        scratch_shapes=[pltpu.SemaphoreType.DMA((len(arrays),))],
        compiler_params=pltpu.CompilerParams(vmem_limit_bytes=4 * 2**20),
        cost_estimate=pl.CostEstimate(flops=COVER, bytes_accessed=2**18, transcendentals=0),
    )(*map(in_hbm, arrays))


def read_kernel(pieces, *refs):
    token_refs, refs = refs[:pieces], refs[pieces:]
    (gain, wi, wf, old_max_t, wq, memory, *refs) = refs
    (normed_out, query_out, old_part, keep_out, admit_out, floor_out, new_max_t, full) = refs
    rows, heads, dim = memory.shape[:3]

    for ref, start in zip(token_refs, piece_starts(token_refs, "tp")):
        full[:, pl.ds(start, ref.shape[1])] = ref[...].astype(F32)
    x = full[...]
    scale = lax.rsqrt(jnp.mean(x * x, axis=1, keepdims=True) + 1e-06)
    normed = (x * scale * gain[...]).astype(BF16)
    normed_out[...] = normed

    def nt(a, b):
        return lax.dot_general(a, b, NT, preferred_element_type=F32)

    all_heads = wi.shape[0]
    me = lax.axis_index("tp")

    def own_heads(x):
        out = x[:heads]
        for i in range(1, all_heads // heads):
            out = jnp.where(me == i, x[i * heads : (i + 1) * heads], out)
        return out

    queries = jnp.dot(normed, wq[...], preferred_element_type=F32) * dim ** (-0.5)
    query_out[...] = queries
    igate = own_heads(nt(wi[...], normed))
    lforget = jax.nn.log_sigmoid(own_heads(nt(wf[...], normed)))
    old_max = old_max_t[...]
    max_t = jnp.maximum(lforget + old_max, igate)
    new_max_t[...] = max_t
    keep_out[...] = jnp.exp(lforget + old_max - max_t).T
    admit_out[...] = jnp.exp(igate - max_t).T
    floor_out[...] = jnp.exp(-max_t).T

    columns = [queries[:, h * dim : (h + 1) * dim].T for h in range(heads)]
    for b in range(rows):
        for h in range(heads):
            part = jnp.sum(memory[b, h] * columns[h][:, b : b + 1], axis=0, keepdims=True)
            old_part[h, b : b + 1, :] = part


def run_read(token_pieces, gain, wi, wf, old_max_t, wq, memory):
    rows, heads, dim = memory.shape[:3]
    depth, inner = wq.shape
    return pl.pallas_call(
        functools.partial(read_kernel, len(token_pieces)),
        name="read",
        out_shape=[
            pltpu.VMEM((rows, depth), BF16),
            pltpu.VMEM((rows, inner), F32),
            pltpu.VMEM((heads, rows, dim), F32),
            pltpu.VMEM((rows, heads), F32),
            pltpu.VMEM((rows, heads), F32),
            pltpu.VMEM((rows, heads), F32),
            jax.ShapeDtypeStruct((heads, rows), F32),
        ],
        in_specs=[VMEM] * (len(token_pieces) + 6),
        out_specs=[VMEM] * 7,
        scratch_shapes=[pltpu.VMEM((rows, depth), F32)],
        compiler_params=pltpu.CompilerParams(vmem_limit_bytes=16 * 2**20),
        cost_estimate=pl.CostEstimate(flops=2**30, bytes_accessed=6 * 2**20, transcendentals=0),
    )(*token_pieces, gain, wi, wf, old_max_t, *map(in_vmem, [wq, memory]))


def mix_kernel(*refs):
    (normed, query, old_part, keep, admit, floor, normalizer, wk, wv, wo, *refs) = refs
    (mixed, new_normalizer, key_out, value_out) = refs
    _, heads, dim = normalizer.shape

    def head(x, h):
        return x[:, h * dim : (h + 1) * dim]

    x = normed[...]
    keys = jnp.dot(x, wk[...], preferred_element_type=F32)
    values = jnp.dot(x, wv[...], preferred_element_type=F32)
    outgate = jax.nn.sigmoid(jnp.dot(x, wo[...], preferred_element_type=F32))
    key_out[...] = keys
    value_out[...] = values
    for h in range(heads):
        q, k, v = head(query[...], h), head(keys, h), head(values, h)
        kw, aw = keep[:, h : h + 1], admit[:, h : h + 1]
        norm = kw * normalizer[:, h, :] + aw * k
        new_normalizer[:, h, :] = norm
        query_key = jnp.sum(q * k, axis=1, keepdims=True)
        denominator = jnp.sum(q * norm, axis=1, keepdims=True)
        numerator = kw * old_part[h] + (aw * query_key) * v
        cell_out = numerator / jnp.maximum(jnp.abs(denominator), floor[:, h : h + 1])
        centered = cell_out - jnp.mean(cell_out, axis=1, keepdims=True)
        variance = jnp.mean(centered * centered, axis=1, keepdims=True)
        gated = head(outgate, h) * centered * lax.rsqrt(variance + 1e-05)
        mixed[:, h * dim : (h + 1) * dim] = gated.astype(BF16)


def run_mix(normed, query, old_part, keep, admit, floor, normalizer, weights):
    rows, heads, dim = normalizer.shape
    depth, inner = weights[0].shape
    flops = 2 * rows * depth * inner * len(weights)
    return pl.pallas_call(
        mix_kernel,
        name="mix",
        out_shape=[
            pltpu.VMEM((rows, inner), BF16),
            jax.ShapeDtypeStruct((rows, heads, dim), F32),
            pltpu.VMEM((rows, inner), F32),
            pltpu.VMEM((rows, inner), F32),
        ],
        in_specs=[VMEM] * 10,
        out_specs=[VMEM] * 4,
        compiler_params=pltpu.CompilerParams(vmem_limit_bytes=16 * 2**20),
        cost_estimate=pl.CostEstimate(flops=flops * 32, bytes_accessed=6 * 2**20, transcendentals=0),
    )(normed, query, old_part, keep, admit, floor, normalizer, *map(in_vmem, weights))


def out_kernel(pieces, *refs):
    mixed_refs, (tokens, w_output, resid) = refs[:pieces], refs[pieces:]
    total = tokens[...].astype(F32)
    for ref, start in zip(mixed_refs, piece_starts(mixed_refs, "tp")):
        weight = w_output[pl.ds(start, ref.shape[1]), :]
        total = total + jnp.dot(ref[...], weight, preferred_element_type=F32)
    resid[...] = total.astype(BF16)


def run_out(mixed_pieces, tokens, w_output):
    rows, width = tokens.shape
    return pl.pallas_call(
        functools.partial(out_kernel, len(mixed_pieces)),
        name="out_projection",
        out_shape=pltpu.VMEM((rows, width), BF16),
        in_specs=[VMEM] * (len(mixed_pieces) + 2),
        out_specs=VMEM,
        compiler_params=pltpu.CompilerParams(vmem_limit_bytes=24 * 2**20),
        cost_estimate=pl.CostEstimate(
            flops=2 * rows * w_output.size, bytes_accessed=2 * w_output.size, transcendentals=0
        ),
    )(*mixed_pieces, tokens, w_output)


def stack_kernel(low, *refs):
    *pieces, out = refs
    me = lax.div(lax.axis_index("kv"), low)
    for step, ref in enumerate(pieces):
        out[partner(me, step, out.shape[0])] = ref[...]


def run_stack(pieces, low):
    return pl.pallas_call(
        functools.partial(stack_kernel, low),
        name="stack",
        out_shape=pltpu.VMEM((len(pieces), *pieces[0].shape), BF16),
        in_specs=[VMEM] * len(pieces),
        out_specs=VMEM,
        compiler_params=pltpu.CompilerParams(vmem_limit_bytes=16 * 2**20),
        cost_estimate=pl.CostEstimate(flops=2**20, bytes_accessed=2**18, transcendentals=0),
    )(*pieces)


def up_kernel(pieces, *refs):
    piece_refs, (gain, w_gate, w_up, own, sent) = refs[:pieces], refs[pieces:]
    hidden = w_gate.shape[0]
    half = own.shape[1] // 2
    x = jnp.concatenate([ref[...].reshape(-1, ref.shape[2]) for ref in piece_refs], axis=0).astype(F32)
    squares = jnp.sum(x * x, axis=1, keepdims=True)
    ffn_in = (x * gain[...]).astype(BF16)
    own[...] = jnp.zeros_like(own)
    for weight, first in [(w_gate, 0), (w_up, half)]:
        own[:, first : first + hidden] = lax.dot_general(ffn_in, weight[...], NT, preferred_element_type=F32)
    lane = lax.broadcasted_iota(jnp.int32, (x.shape[0], LANES), 1)
    high = squares.astype(BF16).astype(F32)
    first = hidden // LANES * LANES
    tile = own[:, first : first + LANES]
    spot = hidden - first
    own[:, first : first + LANES] = jnp.where(lane == spot, squares, tile)
    sent[...] = own[...].astype(BF16)
    tile = jnp.where(lane == spot, high, jnp.where(lane == spot + 1, squares - high, tile))
    sent[:, first : first + LANES] = tile.astype(BF16)


def run_up(pieces, gain, gate_t, up_t):
    rows, depth = sum(x.shape[0] * x.shape[1] for x in pieces), pieces[0].shape[2]
    hidden = gate_t.shape[0]
    half = (hidden + 2 + LANES - 1) // LANES * LANES
    return pl.pallas_call(
        functools.partial(up_kernel, len(pieces)),
        name="gate_up",
        out_shape=[jax.ShapeDtypeStruct((rows, 2 * half), F32), jax.ShapeDtypeStruct((rows, 2 * half), BF16)],
        in_specs=[VMEM] * (len(pieces) + 3),
        out_specs=[VMEM, VMEM],
        compiler_params=pltpu.CompilerParams(vmem_limit_bytes=24 * 2**20),
        cost_estimate=pl.CostEstimate(flops=4 * rows * depth * hidden, bytes_accessed=4 * 2**20, transcendentals=0),
    )(*pieces, gain, gate_t, up_t)


def down_kernel(others, channels, own, *refs):
    other_refs, (w_down, *outs) = refs[:others], refs[others:]
    hidden = w_down.shape[0]
    half = own.shape[1] // 2
    gate, up = own[:, :half], own[:, half:]
    squares = gate[:, hidden : hidden + 1]
    for ref in other_refs:
        theirs = ref[...].astype(F32)
        gate, up = gate + theirs[:, :half], up + theirs[:, half:]
        squares = squares + theirs[:, hidden : hidden + 1] + theirs[:, hidden + 1 : hidden + 2]
    scale = lax.rsqrt(squares / channels + 1e-06)
    gate = scale * gate[:, :hidden]
    act = (gate * jax.nn.sigmoid(gate) * (scale * up[:, :hidden])).astype(BF16)
    full = jnp.dot(act, w_down[...], preferred_element_type=F32).reshape(len(outs), *outs[0].shape)
    for i, ref in enumerate(outs):
        ref[...] = full[i].astype(ref.dtype)


def run_down(own, others, w_down, channels, kind, pieces, high):
    rows = own.shape[0] // (pieces * high)
    hidden, width = w_down.shape
    return pl.pallas_call(
        functools.partial(down_kernel, len(others), channels),
        name="down",
        out_shape=[pltpu.VMEM((high, rows, width), kind)] * pieces,
        in_specs=[VMEM] * (2 + len(others)),
        out_specs=[VMEM] * pieces,
        compiler_params=pltpu.CompilerParams(vmem_limit_bytes=16 * 2**20),
        cost_estimate=pl.CostEstimate(flops=2 * own.shape[0] * width * hidden, bytes_accessed=2**21, transcendentals=0),
    )(own, *others, w_down)


def fold_kernel(count, low, kept, *refs):
    received, (own, *sent), total = refs[:count], refs[count:-1], refs[-1]
    x = kept[...]
    for ref in received:
        x = x + ref[...].astype(F32)
    total[...] = x
    high = kept.shape[0]
    me = lax.div(lax.axis_index("kv"), low)
    own[...] = total[me]
    for step, ref in enumerate(sent, 1):
        ref[...] = total[partner(me, step, high)].astype(BF16)


def run_fold(kept, received, low):
    high, rows, width = kept.shape
    return pl.pallas_call(
        functools.partial(fold_kernel, len(received), low),
        name="fold",
        out_shape=[pltpu.VMEM((rows, width), F32)] + [pltpu.VMEM((rows, width), BF16)] * (high - 1),
        in_specs=[VMEM] * (1 + len(received)),
        out_specs=[VMEM] * high,
        scratch_shapes=[pltpu.VMEM(kept.shape, F32)],
        compiler_params=pltpu.CompilerParams(vmem_limit_bytes=16 * 2**20),
        cost_estimate=pl.CostEstimate(flops=2**24, bytes_accessed=2**20, transcendentals=0),
    )(kept, *received)


def make(kv, tp):
    def per_device(
        tokens,
        norm_gain,
        w_query,
        w_key,
        w_value,
        w_outgate,
        w_input_gate,
        w_forget_gate,
        memory,
        normalizer,
        memory_max,
        w_output,
        ffn_gain,
        w_gate,
        w_up,
        w_down,
    ):
        rows, own_channels = tokens.shape
        heads, head_dim = memory.shape[1], memory.shape[2]
        own, gain, wi, wf, old_normalizer, old_max_t = load(
            [tokens, norm_gain[None], w_input_gate.T, w_forget_gate.T, normalizer, memory_max.T]
        )
        pieces = column_pieces(own, "tp", tp)
        normed, query, old_part, keep, admit, floor, new_max_t = run_read(
            pieces, gain, wi, wf, old_max_t, w_query, memory
        )
        mixed, new_normalizer, keys, values = run_mix(
            normed, query, old_part, keep, admit, floor, old_normalizer, [w_key, w_value, w_outgate]
        )
        pieces = column_pieces(mixed, "tp", tp)
        resid = run_out(pieces, tokens, w_output)
        high, low = group_sizes(kv)
        column = [resid] + staged([resid] * (high - 1), kv, low, False)
        block = run_stack(column, low)
        every_row = [block] + staged([block] * (low - 1), kv, low, True)
        by_head = (rows, heads, head_dim)
        outer = keys.reshape(by_head)[..., :, None] * values.reshape(by_head)[..., None, :]
        new_memory = keep[..., None, None] * memory + admit[..., None, None] * outer
        gain, gate_t, up_t = ffn_gain[None], w_gate.T, w_up.T

        def mixer(group, kind):
            own, sent = run_up(group, gain, gate_t, up_t)
            others = [shifted(sent, "tp", tp, step) for step in range(1, tp)]
            return run_down(own, others, w_down, own_channels * tp, kind, len(group), high)

        (kept,) = mixer(every_row[:1], F32)
        sent = mixer(every_row[1:], BF16) if low > 1 else []
        received = staged(sent, kv, low, True)
        kept, *sent = run_fold(kept, received, low)
        received = staged(sent, kv, low, False)
        down_out = kept
        for x in received:
            down_out = down_out + x.astype(F32)
        result = (resid.astype(F32) + down_out).astype(BF16)
        return (result, new_memory, new_normalizer, new_max_t.T)

    return per_device


def solution(mesh):
    placed = (
        P("kv", "tp"),
        P(),
        P(None, "tp"),
        P(None, "tp"),
        P(None, "tp"),
        P(None, "tp"),
        P(),
        P(),
        P("kv", "tp", None, None),
        P("kv", "tp", None),
        P("kv", "tp"),
        P(None, "tp"),
        P("tp"),
        P("tp", "kv"),
        P("tp", "kv"),
        P("kv", "tp"),
    )
    body = make(mesh.shape["kv"], mesh.shape["tp"])

    return jax.shard_map(
        body,
        mesh=mesh,
        in_specs=placed,
        out_specs=(P("kv", "tp"), P("kv", "tp", None, None), P("kv", "tp", None), P("kv", "tp")),
        check_vma=False,
    )
```

```python
import functools

import jax
import jax.numpy as jnp
from jax import lax
from jax.experimental import pallas as pl
from jax.experimental.pallas import tpu as pltpu
from jax.sharding import PartitionSpec as P


BF16 = jnp.bfloat16
F32 = jnp.float32
LANES = 128
COVER = 2**36
HBM = pl.BlockSpec(memory_space=pltpu.HBM)
VMEM = pl.BlockSpec(memory_space=pltpu.VMEM)
NT = (((1,), (1,)), ((), ()))


def shifted(x, axis, size, step):
    return lax.ppermute(x, axis, [(i, (i + step) % size) for i in range(size)])


def partner(i, step, size):
    return i ^ step if size & (size - 1) == 0 else (i + step) % size


def group_sizes(size):
    low = 1
    while low * low < size:
        low *= 2
    return (size // low, low) if size % low == 0 else (size, 1)


def exchange(x, axis, size, low, step, inner):
    pairs = []
    for k in range(size):
        a, b = divmod(k, low)
        b2 = partner(b, step, low) if inner else b
        a2 = a if inner else partner(a, step, size // low)
        pairs.append((k, a2 * low + b2))
    return lax.ppermute(x, axis, pairs)


def staged(sent, size, low, inner):
    received = []
    for step, x in enumerate(sent, 1):
        received.append(exchange(x, "kv", size, low, step, inner))
    return received


def column_pieces(x, axis, size):
    if size != 2:
        return [lax.all_gather(x, axis, axis=1, tiled=True)]
    return [x, shifted(x, axis, size, 1)]


def in_vmem(x):
    return pltpu.with_memory_space_constraint(x, pltpu.VMEM)


def in_hbm(x):
    return pltpu.with_memory_space_constraint(x, pltpu.HBM)


def piece_starts(refs, axis):
    if len(refs) == 1:
        return [0]
    me, width = lax.axis_index(axis), refs[0].shape[1]
    return [pl.multiple_of(me * width, LANES), pl.multiple_of((1 - me) * width, LANES)]


def load_kernel(count, *refs):
    sources, targets, sem = refs[:count], refs[count : 2 * count], refs[-1]
    copies = [pltpu.make_async_copy(a, b, sem.at[i]) for i, (a, b) in enumerate(zip(sources, targets))]
    for copy in copies:
        copy.start()
    for copy in copies:
        copy.wait()


def load(arrays):
    return pl.pallas_call(
        functools.partial(load_kernel, len(arrays)),
        name="load",
        out_shape=[pltpu.VMEM(x.shape, x.dtype) for x in arrays],
        in_specs=[HBM] * len(arrays),
        out_specs=[VMEM] * len(arrays),
        scratch_shapes=[pltpu.SemaphoreType.DMA((len(arrays),))],
        compiler_params=pltpu.CompilerParams(vmem_limit_bytes=4 * 2**20),
        cost_estimate=pl.CostEstimate(flops=COVER, bytes_accessed=2**18, transcendentals=0),
    )(*map(in_hbm, arrays))


def read_kernel(pieces, *refs):
    token_refs, refs = refs[:pieces], refs[pieces:]
    (gain, wi, wf, old_max_t, wq, memory, *refs) = refs
    (normed_out, query_out, old_part, keep_out, admit_out, floor_out, new_max_t, full) = refs
    rows, heads, dim = memory.shape[:3]

    for ref, start in zip(token_refs, piece_starts(token_refs, "tp")):
        full[:, pl.ds(start, ref.shape[1])] = ref[...].astype(F32)
    x = full[...]
    scale = lax.rsqrt(jnp.mean(x * x, axis=1, keepdims=True) + 1e-06)
    normed = (x * scale * gain[...]).astype(BF16)
    normed_out[...] = normed

    def nt(a, b):
        return lax.dot_general(a, b, NT, preferred_element_type=F32)

    all_heads = wi.shape[0]
    me = lax.axis_index("tp")

    def own_heads(x):
        out = x[:heads]
        for i in range(1, all_heads // heads):
            out = jnp.where(me == i, x[i * heads : (i + 1) * heads], out)
        return out

    queries = jnp.dot(normed, wq[...], preferred_element_type=F32) * dim ** (-0.5)
    query_out[...] = queries
    igate = own_heads(nt(wi[...], normed))
    lforget = jax.nn.log_sigmoid(own_heads(nt(wf[...], normed)))
    old_max = old_max_t[...]
    max_t = jnp.maximum(lforget + old_max, igate)
    new_max_t[...] = max_t
    keep_out[...] = jnp.exp(lforget + old_max - max_t).T
    admit_out[...] = jnp.exp(igate - max_t).T
    floor_out[...] = jnp.exp(-max_t).T

    columns = [queries[:, h * dim : (h + 1) * dim].T for h in range(heads)]
    for b in range(rows):
        for h in range(heads):
            part = jnp.sum(memory[b, h] * columns[h][:, b : b + 1], axis=0, keepdims=True)
            old_part[h, b : b + 1, :] = part


def run_read(token_pieces, gain, wi, wf, old_max_t, wq, memory):
    rows, heads, dim = memory.shape[:3]
    depth, inner = wq.shape
    return pl.pallas_call(
        functools.partial(read_kernel, len(token_pieces)),
        name="read",
        out_shape=[
            pltpu.VMEM((rows, depth), BF16),
            pltpu.VMEM((rows, inner), F32),
            pltpu.VMEM((heads, rows, dim), F32),
            pltpu.VMEM((rows, heads), F32),
            pltpu.VMEM((rows, heads), F32),
            pltpu.VMEM((rows, heads), F32),
            jax.ShapeDtypeStruct((heads, rows), F32),
        ],
        in_specs=[VMEM] * (len(token_pieces) + 6),
        out_specs=[VMEM] * 7,
        scratch_shapes=[pltpu.VMEM((rows, depth), F32)],
        compiler_params=pltpu.CompilerParams(vmem_limit_bytes=16 * 2**20),
        cost_estimate=pl.CostEstimate(flops=2**30, bytes_accessed=6 * 2**20, transcendentals=0),
    )(*token_pieces, gain, wi, wf, old_max_t, *map(in_vmem, [wq, memory]))


def mix_kernel(*refs):
    (normed, query, old_part, keep, admit, floor, normalizer, wk, wv, wo, *refs) = refs
    (mixed, new_normalizer, key_out, value_out) = refs
    _, heads, dim = normalizer.shape

    def head(x, h):
        return x[:, h * dim : (h + 1) * dim]

    x = normed[...]
    keys = jnp.dot(x, wk[...], preferred_element_type=F32)
    values = jnp.dot(x, wv[...], preferred_element_type=F32)
    outgate = jax.nn.sigmoid(jnp.dot(x, wo[...], preferred_element_type=F32))
    key_out[...] = keys
    value_out[...] = values
    for h in range(heads):
        q, k, v = head(query[...], h), head(keys, h), head(values, h)
        kw, aw = keep[:, h : h + 1], admit[:, h : h + 1]
        norm = kw * normalizer[:, h, :] + aw * k
        new_normalizer[:, h, :] = norm
        query_key = jnp.sum(q * k, axis=1, keepdims=True)
        denominator = jnp.sum(q * norm, axis=1, keepdims=True)
        numerator = kw * old_part[h] + (aw * query_key) * v
        cell_out = numerator / jnp.maximum(jnp.abs(denominator), floor[:, h : h + 1])
        centered = cell_out - jnp.mean(cell_out, axis=1, keepdims=True)
        variance = jnp.mean(centered * centered, axis=1, keepdims=True)
        gated = head(outgate, h) * centered * lax.rsqrt(variance + 1e-05)
        mixed[:, h * dim : (h + 1) * dim] = gated.astype(BF16)


def run_mix(normed, query, old_part, keep, admit, floor, normalizer, weights):
    rows, heads, dim = normalizer.shape
    depth, inner = weights[0].shape
    flops = 2 * rows * depth * inner * len(weights)
    return pl.pallas_call(
        mix_kernel,
        name="mix",
        out_shape=[
            pltpu.VMEM((rows, inner), BF16),
            jax.ShapeDtypeStruct((rows, heads, dim), F32),
            pltpu.VMEM((rows, inner), F32),
            pltpu.VMEM((rows, inner), F32),
        ],
        in_specs=[VMEM] * 10,
        out_specs=[VMEM] * 4,
        compiler_params=pltpu.CompilerParams(vmem_limit_bytes=16 * 2**20),
        cost_estimate=pl.CostEstimate(flops=flops * 32, bytes_accessed=6 * 2**20, transcendentals=0),
    )(normed, query, old_part, keep, admit, floor, normalizer, *map(in_vmem, weights))


def out_kernel(pieces, *refs):
    mixed_refs, (tokens, w_output, resid) = refs[:pieces], refs[pieces:]
    total = tokens[...].astype(F32)
    for ref, start in zip(mixed_refs, piece_starts(mixed_refs, "tp")):
        weight = w_output[pl.ds(start, ref.shape[1]), :]
        total = total + jnp.dot(ref[...], weight, preferred_element_type=F32)
    resid[...] = total.astype(BF16)


def run_out(mixed_pieces, tokens, w_output):
    rows, width = tokens.shape
    return pl.pallas_call(
        functools.partial(out_kernel, len(mixed_pieces)),
        name="out_projection",
        out_shape=pltpu.VMEM((rows, width), BF16),
        in_specs=[VMEM] * (len(mixed_pieces) + 2),
        out_specs=VMEM,
        compiler_params=pltpu.CompilerParams(vmem_limit_bytes=24 * 2**20),
        cost_estimate=pl.CostEstimate(
            flops=2 * rows * w_output.size, bytes_accessed=2 * w_output.size, transcendentals=0
        ),
    )(*mixed_pieces, tokens, w_output)


def stack_kernel(low, *refs):
    *pieces, out = refs
    me = lax.div(lax.axis_index("kv"), low)
    for step, ref in enumerate(pieces):
        out[partner(me, step, out.shape[0])] = ref[...]


def run_stack(pieces, low):
    return pl.pallas_call(
        functools.partial(stack_kernel, low),
        name="stack",
        out_shape=pltpu.VMEM((len(pieces), *pieces[0].shape), BF16),
        in_specs=[VMEM] * len(pieces),
        out_specs=VMEM,
        compiler_params=pltpu.CompilerParams(vmem_limit_bytes=16 * 2**20),
        cost_estimate=pl.CostEstimate(flops=2**20, bytes_accessed=2**18, transcendentals=0),
    )(*pieces)


def up_kernel(pieces, *refs):
    piece_refs, (gain, w_gate, w_up, own, sent) = refs[:pieces], refs[pieces:]
    hidden = w_gate.shape[0]
    half = own.shape[1] // 2
    x = jnp.concatenate([ref[...].reshape(-1, ref.shape[2]) for ref in piece_refs], axis=0).astype(F32)
    squares = jnp.sum(x * x, axis=1, keepdims=True)
    ffn_in = (x * gain[...]).astype(BF16)
    lane = lax.broadcasted_iota(jnp.int32, (x.shape[0], LANES), 1)
    high = squares.astype(BF16).astype(F32)
    whole = hidden // LANES * LANES
    spot = hidden - whole
    blank = jnp.zeros((x.shape[0], half - hidden), F32)
    for weight, first in [(w_gate, 0), (w_up, half)]:
        part = lax.dot_general(ffn_in, weight[...], NT, preferred_element_type=F32)
        part = jnp.concatenate([part, blank], axis=1)
        own[:, first : first + half] = part
        sent[:, first : first + half] = part.astype(BF16)
        if not first:
            tile = part[:, whole : whole + LANES]
    own[:, whole : whole + LANES] = jnp.where(lane == spot, squares, tile)
    tile = jnp.where(lane == spot, high, jnp.where(lane == spot + 1, squares - high, tile))
    sent[:, whole : whole + LANES] = tile.astype(BF16)


def run_up(pieces, gain, gate_t, up_t):
    rows, depth = sum(x.shape[0] * x.shape[1] for x in pieces), pieces[0].shape[2]
    hidden = gate_t.shape[0]
    half = (hidden + 2 + LANES - 1) // LANES * LANES
    return pl.pallas_call(
        functools.partial(up_kernel, len(pieces)),
        name="gate_up",
        out_shape=[jax.ShapeDtypeStruct((rows, 2 * half), F32), jax.ShapeDtypeStruct((rows, 2 * half), BF16)],
        in_specs=[VMEM] * (len(pieces) + 3),
        out_specs=[VMEM, VMEM],
        compiler_params=pltpu.CompilerParams(vmem_limit_bytes=24 * 2**20),
        cost_estimate=pl.CostEstimate(flops=4 * rows * depth * hidden, bytes_accessed=4 * 2**20, transcendentals=0),
    )(*pieces, gain, gate_t, up_t)


def down_kernel(others, channels, own, *refs):
    other_refs, (w_down, *outs) = refs[:others], refs[others:]
    hidden = w_down.shape[0]
    half = own.shape[1] // 2
    gate, up = own[:, :half], own[:, half:]
    squares = gate[:, hidden : hidden + 1]
    for ref in other_refs:
        theirs = ref[...].astype(F32)
        gate, up = gate + theirs[:, :half], up + theirs[:, half:]
        squares = squares + theirs[:, hidden : hidden + 1] + theirs[:, hidden + 1 : hidden + 2]
    scale = lax.rsqrt(squares / channels + 1e-06)
    gate = scale * gate[:, :hidden]
    act = (gate * jax.nn.sigmoid(gate) * (scale * up[:, :hidden])).astype(BF16)
    full = jnp.dot(act, w_down[...], preferred_element_type=F32).reshape(len(outs), *outs[0].shape)
    for i, ref in enumerate(outs):
        ref[...] = full[i].astype(ref.dtype)


def run_down(own, others, w_down, channels, kind, pieces, high):
    rows = own.shape[0] // (pieces * high)
    hidden, width = w_down.shape
    return pl.pallas_call(
        functools.partial(down_kernel, len(others), channels),
        name="down",
        out_shape=[pltpu.VMEM((high, rows, width), kind)] * pieces,
        in_specs=[VMEM] * (2 + len(others)),
        out_specs=[VMEM] * pieces,
        compiler_params=pltpu.CompilerParams(vmem_limit_bytes=16 * 2**20),
        cost_estimate=pl.CostEstimate(flops=2 * own.shape[0] * width * hidden, bytes_accessed=2**21, transcendentals=0),
    )(own, *others, w_down)


def fold_kernel(count, low, kept, *refs):
    received, (own, *sent), total = refs[:count], refs[count:-1], refs[-1]
    x = kept[...]
    for ref in received:
        x = x + ref[...].astype(F32)
    total[...] = x
    high = kept.shape[0]
    me = lax.div(lax.axis_index("kv"), low)
    own[...] = total[me]
    for step, ref in enumerate(sent, 1):
        ref[...] = total[partner(me, step, high)].astype(BF16)


def run_fold(kept, received, low):
    high, rows, width = kept.shape
    return pl.pallas_call(
        functools.partial(fold_kernel, len(received), low),
        name="fold",
        out_shape=[pltpu.VMEM((rows, width), F32)] + [pltpu.VMEM((rows, width), BF16)] * (high - 1),
        in_specs=[VMEM] * (1 + len(received)),
        out_specs=[VMEM] * high,
        scratch_shapes=[pltpu.VMEM(kept.shape, F32)],
        compiler_params=pltpu.CompilerParams(vmem_limit_bytes=16 * 2**20),
        cost_estimate=pl.CostEstimate(flops=2**24, bytes_accessed=2**20, transcendentals=0),
    )(kept, *received)


def make(kv, tp):
    def per_device(
        tokens,
        norm_gain,
        w_query,
        w_key,
        w_value,
        w_outgate,
        w_input_gate,
        w_forget_gate,
        memory,
        normalizer,
        memory_max,
        w_output,
        ffn_gain,
        w_gate,
        w_up,
        w_down,
    ):
        rows, own_channels = tokens.shape
        heads, head_dim = memory.shape[1], memory.shape[2]
        own, gain, wi, wf, old_normalizer, old_max_t = load(
            [tokens, norm_gain[None], w_input_gate.T, w_forget_gate.T, normalizer, memory_max.T]
        )
        pieces = column_pieces(own, "tp", tp)
        normed, query, old_part, keep, admit, floor, new_max_t = run_read(
            pieces, gain, wi, wf, old_max_t, w_query, memory
        )
        mixed, new_normalizer, keys, values = run_mix(
            normed, query, old_part, keep, admit, floor, old_normalizer, [w_key, w_value, w_outgate]
        )
        pieces = column_pieces(mixed, "tp", tp)
        resid = run_out(pieces, tokens, w_output)
        high, low = group_sizes(kv)
        column = [resid] + staged([resid] * (high - 1), kv, low, False)
        block = run_stack(column, low)
        every_row = [block] + staged([block] * (low - 1), kv, low, True)
        by_head = (rows, heads, head_dim)
        outer = keys.reshape(by_head)[..., :, None] * values.reshape(by_head)[..., None, :]
        new_memory = keep[..., None, None] * memory + admit[..., None, None] * outer
        gain, gate_t, up_t = ffn_gain[None], w_gate.T, w_up.T

        def mixer(group, kind):
            own, sent = run_up(group, gain, gate_t, up_t)
            others = [shifted(sent, "tp", tp, step) for step in range(1, tp)]
            return run_down(own, others, w_down, own_channels * tp, kind, len(group), high)

        (kept,) = mixer(every_row[:1], F32)
        sent = mixer(every_row[1:], BF16) if low > 1 else []
        received = staged(sent, kv, low, True)
        kept, *sent = run_fold(kept, received, low)
        received = staged(sent, kv, low, False)
        down_out = kept
        for x in received:
            down_out = down_out + x.astype(F32)
        result = (resid.astype(F32) + down_out).astype(BF16)
        return (result, new_memory, new_normalizer, new_max_t.T)

    return per_device


def solution(mesh):
    placed = (
        P("kv", "tp"),
        P(),
        P(None, "tp"),
        P(None, "tp"),
        P(None, "tp"),
        P(None, "tp"),
        P(),
        P(),
        P("kv", "tp", None, None),
        P("kv", "tp", None),
        P("kv", "tp"),
        P(None, "tp"),
        P("tp"),
        P("tp", "kv"),
        P("tp", "kv"),
        P("kv", "tp"),
    )
    body = make(mesh.shape["kv"], mesh.shape["tp"])

    return jax.shard_map(
        body,
        mesh=mesh,
        in_specs=placed,
        out_specs=(P("kv", "tp"), P("kv", "tp", None, None), P("kv", "tp", None), P("kv", "tp")),
        check_vma=False,
    )
```
